32 devices in a mesh: pp: 2 (over x), fs: 4 (over y, core), tp: 4 (over z).
Axes of the slice: x: 2, y: 2, z: 4, core: 2. Of those that a mesh axis runs over, the one named last changes fastest.
Arguments:
- inputs: bfloat16 [512, 2048], P('pp', ('fs', 'tp')), may hold values from -6 to 6
- norm_gain: bfloat16 [2, 2048], P('pp', ('fs', 'tp')), may hold values from 0.099609375 to 1.8984375
- w_value: bfloat16 [2, 2048, 2048], P('pp', None, ('fs', 'tp')), may hold values from -0.125 to 0.125
- w_gate: bfloat16 [2, 2048, 2048], P('pp', None, ('fs', 'tp')), may hold values from -0.125 to 0.125
- w_taps: bfloat16 [2, 31, 2048], P('pp', None, ('fs', 'tp')), may hold values from -1 to 1
- ln_gain: float32 [2, 2048], P('pp', ('fs', 'tp')), may hold values from 0.1 to 1.9
- ln_shift: float32 [2, 2048], P('pp', ('fs', 'tp')), may hold values from -3 to 3
Outputs:
- outputs: bfloat16 [512, 2048], P('pp', ('fs', 'tp'))
The draws below stay inside these ranges and needn't reach their ends.
All inputs are finite; a program needn't handle non-finite values.
Results may differ from the reference program's by a relative error of at most 0.0085.
Values may be sent and summed in bfloat16 or wider, within the bound.
A program may use at most 64 MiB of HBM per device.

```python
import jax
import jax.numpy as jnp
from jax import lax

D = 2048
CONV_W = 31
LEN = 128
MICRO = 4
SECTIONS = 2
TOKENS = 512


def block_scale(rng, dims, pieces, low, high):
    factor_of, own = 1.0, jax.random.fold_in(rng, 6)
    for axis_at, parts in pieces:
        heights = jnp.exp(jax.random.uniform(jax.random.fold_in(own, axis_at), (parts,), jnp.float32, low / len(pieces), high / len(pieces)))
        factor_of = factor_of * jnp.repeat(heights, dims[axis_at] // parts).reshape([-1 if axis == axis_at else 1 for axis in range(len(dims))])
    return factor_of


def bell_draw(stream_key, dims, width, most, split=(), kind=jnp.bfloat16):
    array = jax.random.normal(stream_key, dims, jnp.float32) * width
    if len(split) > 0:
        array = block_scale(stream_key, dims, split, -0.22, 0.18) * array
    return jnp.clip(array, min=-most, max=most).astype(kind)


def setup_inputs(seed: int = 0) -> dict:
    key_of = jax.random.split(jax.random.key(seed), 8)
    inputs = bell_draw(key_of[0], (TOKENS, D), 1.0, 6.0, ((0, 2), (1, 16)))
    norm_gain = jnp.clip(1.0 + 0.18 * jax.random.normal(key_of[1], (SECTIONS, D), jnp.float32), 0.099609375, 1.8984375).astype(jnp.bfloat16)
    w_value = bell_draw(key_of[2], (SECTIONS, D, D), D ** -0.5, 0.125, ((0, 2), (2, 16)))
    w_gate = bell_draw(key_of[3], (SECTIONS, D, D), D ** -0.5, 0.125, ((0, 2), (2, 16)))
    w_taps = bell_draw(key_of[4], (SECTIONS, CONV_W, D), CONV_W ** -0.5, 1.0, ((0, 2), (2, 16)))
    ln_gain = jnp.clip(1.0 + 0.18 * jax.random.normal(key_of[5], (SECTIONS, D), jnp.float32), 0.1, 1.9)
    ln_shift = bell_draw(key_of[6], (SECTIONS, D), 0.5, 3.0, ((0, 2), (1, 16)), jnp.float32)
    return dict(inputs=inputs, norm_gain=norm_gain, w_value=w_value, w_gate=w_gate, w_taps=w_taps, ln_gain=ln_gain, ln_shift=ln_shift)


def section_layer(stream, params):
    norm_gain, w_value, w_gate, w_taps, ln_gain, ln_shift = params
    stream_f = stream.astype(jnp.float32)
    scale_rows = lax.rsqrt(lax.optimization_barrier(jnp.mean(stream_f * stream_f, axis=-1, keepdims=True)) + 1e-06)
    normed = (stream_f * scale_rows * norm_gain.astype(jnp.float32)).astype(jnp.bfloat16)
    flat = normed.reshape(MICRO * LEN, D)
    value_sum = jnp.dot(flat, w_value, preferred_element_type=jnp.float32).reshape(MICRO, LEN, D)
    gate_sum = jnp.dot(flat, w_gate, preferred_element_type=jnp.float32).reshape(MICRO, LEN, D)
    gated_rows = value_sum * jax.nn.sigmoid(gate_sum)
    padded = jnp.pad(gated_rows, ((0, 0), (CONV_W - 1, 0), (0, 0)))
    tap_weights = w_taps.astype(jnp.float32)
    convolved = jnp.zeros((MICRO, LEN, D), jnp.float32)
    for tap_index in range(CONV_W):
        convolved = convolved + padded[:, tap_index:tap_index + LEN] * tap_weights[tap_index]
    row_mean = lax.optimization_barrier(jnp.mean(convolved, axis=-1, keepdims=True))
    row_var = lax.optimization_barrier(jnp.mean(convolved * convolved, axis=-1, keepdims=True)) - row_mean * row_mean
    normed_conv = (convolved - row_mean) * lax.rsqrt(row_var + 1e-05) * ln_gain + ln_shift
    new_stream = (stream_f + jax.nn.silu(normed_conv)).astype(jnp.bfloat16)
    return (new_stream, None)

def reference(inputs, norm_gain, w_value, w_gate, w_taps, ln_gain, ln_shift):
    stream = inputs.reshape(MICRO, LEN, D)
    stream, unused = lax.scan(section_layer, stream, (norm_gain, w_value, w_gate, w_taps, ln_gain, ln_shift))
    return stream.reshape(MICRO * LEN, D)
```

```python
import functools

import jax
import jax.numpy as jnp
from jax import lax
from jax.experimental import pallas as pl
from jax.experimental.pallas import tpu as pltpu
from jax.sharding import PartitionSpec as P

LEN = 128
CHUNK = 64
LAGS = (0, 1, 2)
AHEAD = 4

norm_eps = 1e-06
layer_eps = 1e-05
MESH = pl.DeviceIdType.MESH


def kernel(
    sizes,
    x_hbm,
    gain_hbm,
    wv_hbm,
    wg_hbm,
    taps_hbm,
    lgain_hbm,
    lshift_hbm,
    out_ref,
    x_ref,
    gain_ref,
    wcat,
    taps_ref,
    lgain_ref,
    lshift_ref,
    load_sem,
    sg,
    cg,
    hb,
    gains,
    lng,
    lnb,
    sin,
    sfin,
    sout,
    pad,
    taps,
    conv_own,
    conv_out,
    s_own,
    new_buf,
    turn,
    s_sem,
    c_sem,
    sin_sem,
    sfin_sem,
    gain_sem,
    out_sem,
    feed_send,
    relay_send,
    small_send,
    stat_send,
    next_send,
    back_send,
):
    P_, F, T = sizes
    G = F * T
    k, f, t = lax.axis_index("pp"), lax.axis_index("fs"), lax.axis_index("tp")
    NC, R, C = conv_own.shape
    D = wcat.shape[0]
    W = taps.shape[0]
    own_rows = x_ref.shape[0]
    per_owner = own_rows // R
    per_seq = LEN // R
    head = pad.shape[0] - LEN
    me = f * T + t
    feeds = min(2, P_)

    loads = [
        pltpu.make_async_copy(a, b, load_sem.at[n])
        for n, (a, b) in enumerate(
            [
                (x_hbm, x_ref), (gain_hbm, gain_ref), (lgain_hbm, lgain_ref), (lshift_hbm, lshift_ref),
                (taps_hbm, taps_ref),
                (wv_hbm.at[0], wcat.at[:, pl.ds(0, C)]), (wg_hbm.at[0], wcat.at[:, pl.ds(C, C)]),
            ]
        )
    ]
    for load in loads:
        load.start()

    def own_copies():
        for i in range(per_owner):
            n = k * per_owner + i
            pltpu.make_async_copy(x_hbm.at[pl.ds(i * R, R)], sg.at[n, me], s_sem.at[n, me]).start()

    if P_ > 2:
        pl.when(k < feeds)(own_copies)
    else:
        own_copies()

    if T & (T - 1) == 0:
        to_t = [t] + [t ^ d for d in range(1, T)]
        from_t = to_t
    else:
        to_t = [lax.rem(t + d, T) for d in range(T)]
        from_t = [lax.rem(t + T - d, T) for d in range(T)]

    def at(kk, ff, tt):
        return {"pp": kk, "fs": ff, "tp": tt}

    def send(src, dst, s_sem_, r_sem, dev):
        pltpu.make_async_remote_copy(
            src_ref=src, dst_ref=dst, send_sem=s_sem_, recv_sem=r_sem, device_id=dev, device_id_type=MESH
        ).start()

    def await_bytes(ref, sem):
        pltpu.make_async_copy(ref, ref, sem).wait()

    peers = [at(k, lax.rem(f + df, F), to_t[dt]) for dt in range(T - 1, -1, -1) for df in range(F) if df or dt]

    def plane(kk):
        return [at(kk, lax.rem(f + df, F), to_t[dt]) for dt in range(T - 1, -1, -1) for df in range(F)]

    barrier = pltpu.get_barrier_semaphore()
    everyone = peers + [dev for dk in range(1, P_) for dev in plane(lax.rem(k + dk, P_))]
    for dev in everyone:
        pl.semaphore_signal(barrier, inc=1, device_id=dev, device_id_type=MESH)
    for load in loads[:4]:
        load.wait()
    gains[me] = gain_ref[...].astype(jnp.float32)
    lgain_ref[...] = lgain_ref[...] * 0.5
    lshift_ref[...] = lshift_ref[...] * 0.5
    pad[0:head, :] = jnp.zeros((head, C), jnp.float32)
    turn[...] = jnp.zeros_like(turn)
    pl.semaphore_wait(barrier, len(everyone))

    for q in range(feeds):
        for i in range(per_owner):
            n = k * per_owner + i
            src = x_ref.at[pl.ds(i * R, R)]
            for dt in range(T - 1, 0, -1):
                send(src, sg.at[n, me], feed_send.at[0], s_sem.at[n, me], at(q, f, to_t[dt]))
            if P_ > 1:
                @pl.when(k != q)
                def _():
                    send(src, sg.at[n, me], feed_send.at[0], s_sem.at[n, me], at(q, f, t))
            if q == 0 and i == 0:
                for dev in peers:
                    send(gains.at[me], gains.at[me], small_send.at[0], gain_sem.at[0], dev)

    bits = []
    b = F // 2
    while b:
        bits.append(b)
        b //= 2
    levels = [F] + bits

    def hop(buf, sem, n, low):
        for r in range(F):
            if ((r & -r) if r else F) == low:
                for tt in from_t:
                    slot = (f ^ r) * T + tt
                    block = buf.at[n, slot]
                    await_bytes(block, sem.at[n, slot])
                    for b in bits:
                        if b < low:
                            send(block, block, relay_send.at[0], sem.at[n, slot], at(k, f ^ b, t))

    def prepare():
        for load in loads[4:]:
            load.wait()
        taps[...] = taps_ref[0].astype(jnp.float32)
        await_bytes(gains.at[pl.ds(0, G - 1)], gain_sem.at[0])
        for s in range(G):
            turn[s : s + 1, :] = gains[s]
        cols = turn[...].T
        for s in range(G):
            rows = pl.ds(s * C, C)
            wcat[rows, :] = (wcat[rows, :].astype(jnp.float32) * cols[:, s : s + 1]).astype(jnp.bfloat16)

    def moments(ref, n):
        turn[0:2, :] = jnp.sum(ref[n], axis=0)
        cols = turn[...].T
        mu = cols[0:R, 0:1] / D
        var = cols[0:R, 1:2] / D - mu * mu
        return mu, lax.rsqrt(var + layer_eps)

    def enter(n):
        mu, rs = moments(sin, n)
        blocks = []
        for s in range(G):
            half = (cg[n, s].astype(jnp.float32) - mu) * rs * lng[s] + lnb[s]
            new = (sg[n, s].astype(jnp.float32) + (half + half * jnp.tanh(half))).astype(jnp.bfloat16)
            hb[s] = new
            blocks.append(new)
        s_own[n] = hb[me]
        return blocks

    def project(n, blocks):
        squares = jnp.zeros((R, C), jnp.float32)
        for xb in blocks:
            xf = xb.astype(jnp.float32)
            squares = squares + xf * xf
        scale = lax.rsqrt(jnp.sum(squares, axis=1, keepdims=True) / D + norm_eps)
        both = jnp.dot(jnp.concatenate(blocks, axis=1), wcat[...], preferred_element_type=jnp.float32) * scale
        j = (n % per_seq) * R
        pad[head + j : head + j + R, :] = both[:, :C] * (0.5 + 0.5 * jnp.tanh(0.5 * both[:, C:]))
        step = 32
        for r0 in range(0, R, step):
            acc = jnp.zeros((step, C), jnp.float32)
            for w in range(W):
                o = head - (W - 1) + w + j + r0
                acc = acc + pad[o : o + step, :] * taps[w : w + 1, :]
            conv_own[n, r0 : r0 + step, :] = acc
        conv = conv_own[n]
        lane = lax.broadcasted_iota(jnp.int32, (R, LEN), 1)
        s1 = jnp.sum(conv, axis=1, keepdims=True)
        s2 = jnp.sum(conv * conv, axis=1, keepdims=True)
        turn[0:R, :] = jnp.where(lane == 0, s1, jnp.where(lane == 1, s2, 0.0))
        return conv, turn[...].T[0:2, :]

    def pass_on(n, first):
        conv, stat = project(n, [sg[n, s] for s in range(G)] if first else enter(n))
        sout[n] = stat
        conv_out[n] = conv.astype(jnp.bfloat16)
        if not first:
            for tt in to_t[::-1]:
                send(s_own.at[n], sg.at[n, me], next_send.at[0], s_sem.at[n, me], at(k + 1, f, tt))
        for dev in plane(k + 1):
            send(sout.at[n], sin.at[n, me], stat_send.at[0], sin_sem.at[n], dev)
        for tt in to_t[::-1]:
            send(conv_out.at[n], cg.at[n, me], next_send.at[0], c_sem.at[n, me], at(k + 1, f, tt))

    def last_stats(n, first):
        _, stat = project(n, [sg[n, s] for s in range(G)] if first else enter(n))
        sfin[n, me] = stat
        for dev in peers:
            send(sfin.at[n, me], sfin.at[n, me], stat_send.at[0], sfin_sem.at[n], dev)

    def finish(n, first):
        await_bytes(sfin.at[n, pl.ds(0, G - 1)], sfin_sem.at[n])
        mu, rs = moments(sfin, n)
        half = (conv_own[n] - mu) * rs * lgain_ref[...] + lshift_ref[...]
        stream = sg[n, me] if first else s_own[n]
        new = (stream.astype(jnp.float32) + (half + half * jnp.tanh(half))).astype(jnp.bfloat16)
        owner, i = n // per_owner, n % per_owner
        rows = pl.ds(i * R, R)
        if owner == P_ - 1:
            out_ref[rows, :] = new
        else:
            new_buf[n] = new
            send(new_buf.at[n], out_ref.at[rows], back_send.at[0], out_sem.at[i], at(owner, f, t))

    def staged(buf, sem, i, upto=None):
        for low, lag in list(zip(levels, LAGS))[:upto]:
            if 0 <= i - lag < NC:
                hop(buf, sem, i - lag, low)

    depth = LAGS[len(levels) - 1]

    def run(first, last):
        step = last_stats if last else pass_on
        if first:
            if not last:
                for dev in plane(k + 1):
                    send(lgain_ref, lng.at[me], small_send.at[1], gain_sem.at[1], dev)
                    send(lshift_ref, lnb.at[me], small_send.at[1], gain_sem.at[2], dev)
            for i in range(NC + depth):
                staged(sg, s_sem, i)
                n = i - depth
                if n == 0:
                    prepare()
                if n >= 0:
                    step(n, True)
                    if last and n >= 2:
                        finish(n - 2, True)
        else:
            if not last:
                for dev in plane(k + 1):
                    send(lgain_ref, lng.at[me], small_send.at[1], gain_sem.at[1], dev)
                    send(lshift_ref, lnb.at[me], small_send.at[1], gain_sem.at[2], dev)
            for i in range(min(AHEAD, NC) + depth):
                staged(sg, s_sem, i)
            prepare()
            await_bytes(lng.at[pl.ds(0, G)], gain_sem.at[1])
            await_bytes(lnb.at[pl.ds(0, G)], gain_sem.at[2])
            for i in range(NC + depth):
                staged(cg, c_sem, i)
                n = i - depth
                if i + min(AHEAD, NC) + depth < NC + depth:
                    staged(sg, s_sem, i + min(AHEAD, NC) + depth)
                if n >= 0:
                    await_bytes(sin.at[n, pl.ds(0, G)], sin_sem.at[n])
                    step(n, False)
                    if last and n >= 2:
                        finish(n - 2, False)
        if last:
            for n in range(max(NC - 2, 0), NC):
                finish(n, first)
        hops = T * (F - 1)
        if hops:
            await_bytes(sg.at[:, pl.ds(0, hops)], relay_send.at[0])
            if not first:
                await_bytes(cg.at[:, pl.ds(0, hops)], relay_send.at[0])
        await_bytes(gains.at[pl.ds(0, G - 1)], small_send.at[0])
        if last:
            await_bytes(sfin.at[:, pl.ds(0, G - 1)], stat_send.at[0])
            for _ in range(per_owner * (P_ - 1)):
                await_bytes(out_ref.at[pl.ds(0, R)], back_send.at[0])
        else:
            await_bytes(sin.at[:, pl.ds(0, G)], stat_send.at[0])
            await_bytes(lng.at[pl.ds(0, G)], small_send.at[1])
            await_bytes(lnb.at[pl.ds(0, G)], small_send.at[1])
            await_bytes(cg.at[:, pl.ds(0, T)], next_send.at[0])
            if not first:
                await_bytes(sg.at[:, pl.ds(0, T)], next_send.at[0])

    if P_ == 1:
        run(True, True)
    else:
        pl.when(k == 0)(lambda: run(True, False))
        pl.when(k == P_ - 1)(lambda: run(False, True))
        if P_ > 2:
            pl.when((k > 0) & (k < P_ - 1))(lambda: run(False, False))

    for _ in range(per_owner):
        await_bytes(sg.at[0, pl.ds(0, feeds * T - 1)], feed_send.at[0])
    if P_ > 2:
        @pl.when(k >= feeds)
        def _():
            await_bytes(x_ref, feed_send.at[0])
    if P_ > 1:
        @pl.when(k < P_ - 1)
        def _():
            for i in range(per_owner):
                await_bytes(out_ref.at[pl.ds(i * R, R)], out_sem.at[i])


def local(sizes, inputs, norm_gain, w_value, w_gate, w_taps, ln_gain, ln_shift):
    P_, F, T = sizes
    G = F * T
    own_rows, C = inputs.shape
    R = min(CHUNK, own_rows)
    NC = own_rows * P_ // R
    D = w_value.shape[1]
    W = w_taps.shape[1]
    head = -(-(W - 1) // 8) * 8
    operands = (inputs, norm_gain, w_value, w_gate, w_taps, ln_gain, ln_shift)
    dma = pltpu.SemaphoreType.DMA
    f32, bf16 = jnp.float32, jnp.bfloat16
    V = pltpu.VMEM
    return pl.pallas_call(
        functools.partial(kernel, sizes),
        out_shape=jax.ShapeDtypeStruct((own_rows, C), bf16),
        in_specs=[pl.BlockSpec(memory_space=pl.ANY)] * 7,
        out_specs=pl.BlockSpec(memory_space=pltpu.VMEM),
        scratch_shapes=[
            V(inputs.shape, bf16), V(norm_gain.shape, bf16), V((D, 2 * C), bf16), V(w_taps.shape, bf16),
            V(ln_gain.shape, f32), V(ln_shift.shape, f32),
            dma((len(operands),)),
            V((NC, G, R, C), bf16), V((NC, G, R, C), bf16), V((G, R, C), bf16),
            V((G, 1, C), f32), V((G, 1, C), f32), V((G, 1, C), f32),
            V((NC, G, 2, LEN), f32), V((NC, G, 2, LEN), f32), V((NC, 2, LEN), f32),
            V((LEN + head, C), f32), V((W, C), f32),
            V((NC, R, C), f32), V((NC, R, C), bf16), V((NC, R, C), bf16), V((NC, R, C), bf16),
            V((LEN, LEN), f32),
            dma((NC, G)), dma((NC, G)), dma((NC,)), dma((NC,)), dma((3,)), dma((own_rows // R,)),
            dma((1,)), dma((1,)), dma((2,)), dma((1,)), dma((1,)), dma((1,)),
        ],
        compiler_params=pltpu.CompilerParams(collective_id=0, has_side_effects=True),
    )(*operands)


def solution(mesh):
    sizes = (mesh.shape["pp"], mesh.shape["fs"], mesh.shape["tp"])
    in_specs = (
        P("pp", ("fs", "tp")),
        P("pp", ("fs", "tp")),
        P("pp", None, ("fs", "tp")),
        P("pp", None, ("fs", "tp")),
        P("pp", None, ("fs", "tp")),
        P("pp", ("fs", "tp")),
        P("pp", ("fs", "tp")),
    )
    out_specs = P("pp", ("fs", "tp"))
    return jax.shard_map(
        functools.partial(local, sizes), mesh=mesh, in_specs=in_specs, out_specs=out_specs,
        check_vma=False,
    )
```

```python
import functools

import jax
import jax.numpy as jnp
from jax import lax
from jax.experimental import pallas as pl
from jax.experimental.pallas import tpu as pltpu
from jax.sharding import PartitionSpec as P

LEN = 128
SPLITS = ((128, 128), (128, 128))
FEED = (2, 3, 1)
SEND = (3, 2, 1, 0)
ENTER = (0, 1, 3, 2)
XCARRY = (1, 2)
ZRELAY = (1, 2)
SWAP = 256
TIMES = ()


norm_eps = 1e-06
layer_eps = 1e-05
MESH = pl.DeviceIdType.MESH


def kernel(
    sizes,
    x_hbm,
    gain_hbm,
    wv_hbm,
    wg_hbm,
    taps_hbm,
    lgain_hbm,
    lshift_hbm,
    out_ref,
    x_ref,
    gain_ref,
    wcat,
    taps_ref,
    lgain_ref,
    lshift_ref,
    load_sem,
    sg,
    cg,
    hg,
    gains,
    lng,
    lnb,
    sin,
    sfin,
    sout,
    pad,
    taps,
    conv_own,
    conv_out,
    keep,
    new_buf,
    turn,
    s_sem,
    c_sem,
    h_sem,
    sin_sem,
    sfin_sem,
    gain_sem,
    out_sem,
    feed_send,
    relay_send,
    small_send,
    stat_send,
    next_send,
    back_send,
    side,
    side_sem,
    swap_send,
):
    P_, F, T = sizes
    G = F * T
    k, f, t = lax.axis_index("pp"), lax.axis_index("fs"), lax.axis_index("tp")
    C = conv_own.shape[1]
    D = wcat.shape[0]
    W = taps.shape[0]
    own_rows = x_ref.shape[0]
    head = pad.shape[0] - LEN
    me = f * T + t
    feeds = min(2, P_)

    loads = [
        pltpu.make_async_copy(a, b, load_sem.at[n])
        for n, (a, b) in enumerate(
            [
                (x_hbm, x_ref), (gain_hbm, gain_ref), (lgain_hbm, lgain_ref), (lshift_hbm, lshift_ref),
                (taps_hbm, taps_ref),
                (wv_hbm.at[0], wcat.at[:, pl.ds(0, C)]), (wg_hbm.at[0], wcat.at[:, pl.ds(C, C)]),
            ]
        )
    ]
    for load in loads:
        load.start()

    if T & (T - 1) == 0:
        to_t = [t] + [t ^ d for d in range(1, T)]
        from_t = to_t
    else:
        to_t = [lax.rem(t + d, T) for d in range(T)]
        from_t = [lax.rem(t + T - d, T) for d in range(T)]

    def at(kk, ff, tt):
        return {"pp": kk, "fs": ff, "tp": tt}

    def send(src, dst, s_sem_, r_sem, dev):
        pltpu.make_async_remote_copy(
            src_ref=src, dst_ref=dst, send_sem=s_sem_, recv_sem=r_sem, device_id=dev, device_id_type=MESH
        ).start()

    def await_bytes(ref, sem):
        pltpu.make_async_copy(ref, ref, sem).wait()

    peers = [at(k, lax.rem(f + df, F), to_t[dt]) for dt in range(T - 1, -1, -1) for df in range(F) if df or dt]

    def plane(kk):
        return [at(kk, lax.rem(f + df, F), to_t[dt]) for dt in range(T - 1, -1, -1) for df in range(F)]

    pow2 = T & (T - 1) == 0
    every = tuple(range(T))
    chunks, cross = plan(sizes, own_rows)
    NCH = len(chunks)
    zrelay = ZRELAY if pow2 and T == 4 else ()

    def rows_of(n):
        return pl.ds(chunks[n][0], chunks[n][1])

    def feed(q, dts, mine):
        for n, start, i in mine:
            size = chunks[n][1] if cross else chunks[0][1]
            for dt in dts:
                send(
                    x_ref.at[pl.ds(i, size)], sg.at[me, pl.ds(start, size)], feed_send.at[0], s_sem.at[n, me],
                    at(q, f, to_t[dt]),
                )

    def own_copies(mine):
        for n, start, i in mine:
            size = chunks[n][1] if cross else chunks[0][1]
            pltpu.make_async_copy(
                x_hbm.at[pl.ds(i, size)], sg.at[me, pl.ds(start, size)], s_sem.at[n, me]
            ).start()

    def mine_of(kk):
        return [(n, c, c % own_rows) for n, (c, _) in enumerate(chunks) if c // own_rows == kk]

    if cross:
        for kk in range(P_):
            pl.when(k == kk)(functools.partial(own_copies, mine_of(kk)))
    else:
        size = chunks[0][1]
        mine = [(k * (own_rows // size) + i, k * own_rows + i * size, i * size) for i in range(own_rows // size)]
        if P_ > feeds:
            pl.when(k < feeds)(functools.partial(own_copies, mine))
        else:
            own_copies(mine)
    barrier = pltpu.get_barrier_semaphore()
    everyone = peers + [dev for dk in range(1, P_) for dev in plane(lax.rem(k + dk, P_))]
    for dev in everyone:
        pl.semaphore_signal(barrier, inc=1, device_id=dev, device_id_type=MESH)
    for load in loads[:4]:
        load.wait()
    gains[me] = gain_ref[...].astype(jnp.float32)
    lgain_ref[...] = lgain_ref[...] * 0.5
    lshift_ref[...] = lshift_ref[...] * 0.5
    pad[0:head, :] = jnp.zeros((head, C), jnp.float32)
    turn[...] = jnp.zeros_like(turn)
    pl.semaphore_wait(barrier, len(everyone))

    def greet():
        for dev in peers:
            send(gains.at[me], gains.at[me], small_send.at[0], gain_sem.at[0], dev)

    bits = []
    b = F // 2
    while b:
        bits.append(b)
        b //= 2
    top = len(bits)
    counts = [0]

    def forward(buf, sem, n, slot, dev):
        block = buf.at[slot, rows_of(n)]
        send(block, block, relay_send.at[0], sem.at[n, slot], dev)
        counts[0] += chunks[n][1]

    def arrived(buf, sem, n, slot):
        await_bytes(buf.at[slot, rows_of(n)], sem.at[n, slot])

    def stage(r):
        return 0 if r == 0 else len(bits) - ((r & -r).bit_length() - 1)

    def hop(buf, sem, n, lv, dts, ups=every, down=True, over=()):
        for r in range(F):
            if stage(r) != lv:
                continue
            for dt in dts:
                slot = (f ^ r) * T + from_t[dt]
                arrived(buf, sem, n, slot)
                for b in bits:
                    if b < ((r & -r) or F) and (dt in ups if b == F // 2 else down):
                        forward(buf, sem, n, slot, at(k, f ^ b, t))
                if dt in over:
                    forward(buf, sem, n, slot, at(1 - k, f, t))

    def prepare(first):
        if not first:
            await_bytes(lng.at[pl.ds(0, G)], gain_sem.at[1])
            await_bytes(lnb.at[pl.ds(0, G)], gain_sem.at[2])
        for load in loads[4:]:
            load.wait()
        taps[...] = taps_ref[0].astype(jnp.float32)
        await_bytes(gains.at[pl.ds(0, G - 1)], gain_sem.at[0])
        for s in range(G):
            turn[s : s + 1, :] = gains[s]
        cols = turn[...].T
        for s in range(G):
            rows = pl.ds(s * C, C)
            wcat[rows, :] = (wcat[rows, :].astype(jnp.float32) * cols[:, s : s + 1]).astype(jnp.bfloat16)

    def moments(ref, n):
        R = chunks[n][1]
        turn[0:2, :] = jnp.sum(ref[n], axis=0)
        cols = turn[...].T
        mu = cols[0:R, 0:1] / D
        var = cols[0:R, 1:2] / D - mu * mu
        return mu, lax.rsqrt(var + layer_eps)

    def layer_end(n, slot, mu, rs):
        half = (cg[slot, rows_of(n)].astype(jnp.float32) - mu) * rs * lng[slot] + lnb[slot]
        hg[slot, rows_of(n)] = (
            sg[slot, rows_of(n)].astype(jnp.float32) + (half + half * jnp.tanh(half))
        ).astype(jnp.bfloat16)

    def enter(n, swapped):
        await_bytes(sin.at[n, pl.ds(0, G)], sin_sem.at[n])
        mu, rs = moments(sin, n)
        if swapped:
            keep[0, 0 : chunks[n][1], :] = jnp.broadcast_to(mu, (chunks[n][1], C))
            keep[1, 0 : chunks[n][1], :] = jnp.broadcast_to(rs, (chunks[n][1], C))
        for dt in (ENTER if len(ENTER) == T else every):
            slot = f * T + from_t[dt]
            if dt or not zrelay:
                arrived(cg, c_sem, n, slot)
            layer_end(n, slot, mu, rs)
            for b in bits:
                if not (swapped and dt == 0 and b == F // 2):
                    forward(hg, h_sem, n, slot, at(k, f ^ b, t))

    def enter_swapped(n):
        slot = (f ^ (F // 2)) * T + t
        arrived(cg, c_sem, n, slot)
        layer_end(n, slot, keep[0, 0 : chunks[n][1], :], keep[1, 0 : chunks[n][1], :])
        for b in bits[1:]:
            forward(hg, h_sem, n, slot, at(k, f ^ b, t))

    def spread(n):
        slot = f * T + t
        arrived(cg, c_sem, n, slot)
        for dz in zrelay:
            forward(cg, c_sem, n, slot, at(k, f, to_t[dz]))

    def project(n, buf):
        start, R = chunks[n]
        blocks = [buf[s, rows_of(n)] for s in range(G)]
        squares = jnp.zeros((R, C), jnp.float32)
        for xb in blocks:
            xf = xb.astype(jnp.float32)
            squares = squares + xf * xf
        scale = lax.rsqrt(jnp.sum(squares, axis=1, keepdims=True) / D + norm_eps)
        both = jnp.dot(jnp.concatenate(blocks, axis=1), wcat[...], preferred_element_type=jnp.float32) * scale
        j = start % LEN
        pad[head + j : head + j + R, :] = both[:, :C] * (0.5 + 0.5 * jnp.tanh(0.5 * both[:, C:]))
        step = 32 if R % 32 == 0 else R
        for r0 in range(0, R, step):
            acc = jnp.zeros((step, C), jnp.float32)
            for w in range(W):
                o = head - (W - 1) + w + j + r0
                acc = acc + pad[o : o + step, :] * taps[w : w + 1, :]
            conv_own[start + r0 : start + r0 + step, :] = acc
        conv = conv_own[start : start + R, :]
        lane = lax.broadcasted_iota(jnp.int32, (R, LEN), 1)
        s1 = jnp.sum(conv, axis=1, keepdims=True)
        s2 = jnp.sum(conv * conv, axis=1, keepdims=True)
        turn[0:R, :] = jnp.where(lane == 0, s1, jnp.where(lane == 1, s2, 0.0))
        return conv, turn[...].T[0:2, :]

    def pass_on(n, first, swapped):
        conv, stat = project(n, sg if first else hg)
        rows = rows_of(n)
        sout[n] = stat
        conv_out[rows, :] = conv.astype(jnp.bfloat16)
        for dt in SEND if len(SEND) == T else every:
            if dt not in zrelay:
                send(conv_out.at[rows], cg.at[me, rows], next_send.at[0], c_sem.at[n, me], at(k + 1, f, to_t[dt]))
        for dev in plane(k + 1):
            send(sout.at[n], sin.at[n, me], stat_send.at[0], sin_sem.at[n], dev)
        if swapped:
            send(conv_out.at[rows], side.at[rows], swap_send.at[0], side_sem.at[n], at(k, f ^ (F // 2), t))
        if not first:
            for tt in to_t:
                send(hg.at[me, rows], sg.at[me, rows], next_send.at[0], s_sem.at[n, me], at(k + 1, f, tt))

    def swap_on(n):
        rows = rows_of(n)
        await_bytes(side.at[rows], side_sem.at[n])
        slot = (f ^ (F // 2)) * T + t
        send(side.at[rows], cg.at[slot, rows], swap_send.at[0], c_sem.at[n, slot], at(k + 1, f, t))

    def last_stats(n, first):
        _, stat = project(n, sg if first else hg)
        sfin[n, me] = stat
        for dev in peers:
            send(sfin.at[n, me], sfin.at[n, me], stat_send.at[0], sfin_sem.at[n], dev)

    def finish(n, first):
        start, R = chunks[n]
        await_bytes(sfin.at[n, pl.ds(0, G - 1)], sfin_sem.at[n])
        mu, rs = moments(sfin, n)
        half = (conv_own[start : start + R, :] - mu) * rs * lgain_ref[...] + lshift_ref[...]
        stream = (sg if first else hg)[me, rows_of(n)]
        new = (stream.astype(jnp.float32) + (half + half * jnp.tanh(half))).astype(jnp.bfloat16)
        owner, i = start // own_rows, start % own_rows
        rows = pl.ds(i, R)
        if owner == P_ - 1:
            out_ref[rows, :] = new
        else:
            new_buf[rows_of(n), :] = new
            send(new_buf.at[rows_of(n)], out_ref.at[rows], back_send.at[0], out_sem.at[0], at(owner, f, t))

    def drain(rows, sem):
        full = sg.shape[1]
        while rows >= full:
            m = min(G, rows // full)
            await_bytes(sg.at[pl.ds(0, m)], sem)
            rows -= m * full
        if rows:
            await_bytes(sg.at[0, pl.ds(0, rows)], sem)

    def run(first, last):
        counts[0] = 0
        kk = 0 if first else 1
        ops = []
        for n, (start, size) in enumerate(chunks):
            own = not cross or start // own_rows == kk
            swapped = cross and F > 1 and start >= SWAP
            at_ = functools.partial(when, chunks, own_rows, cross, kk, n)
            x1 = XCARRY if cross else ()
            zero = (0,) if swapped else ()
            if first:
                if own:
                    ops.append((at_("S0"), functools.partial(hop, sg, s_sem, n, 0, every, over=every if cross else ())))
                else:
                    ups = tuple(d for d in every if d not in x1)
                    ops.append((at_("S0"), functools.partial(hop, sg, s_sem, n, 0, every, ups)))
                for lv in range(1, top + 1):
                    over = zero if own and lv == 1 else ()
                    ops.append((at_("S%d" % min(lv, 2)), functools.partial(hop, sg, s_sem, n, lv, every, over=over)))
            else:
                if cross and own:
                    ups = tuple(sorted(set(x1 + zero)))
                    ops.append((at_("S0"), functools.partial(hop, sg, s_sem, n, 0, every, ups, False, every)))
                    if ups:
                        ops.append((at_("S1"), functools.partial(hop, sg, s_sem, n, 1, ups, (), False, x1)))
                else:
                    ops.append((at_("S0"), functools.partial(hop, sg, s_sem, n, 0, every, (), False)))
                    if swapped:
                        ops.append((at_("S1"), functools.partial(hop, sg, s_sem, n, 1, (0,), (), False)))
                if zrelay:
                    ops.append((at_("C00"), functools.partial(spread, n)))
                ops.append((at_("ent"), functools.partial(enter, n, swapped)))
                if swapped:
                    ops.append((at_("ent2"), functools.partial(enter_swapped, n)))
                for lv in range(1, top + 1):
                    dts = every[1:] if swapped and lv == 1 else every
                    ops.append((at_("C%d" % min(lv, 2)), functools.partial(hop, hg, h_sem, n, lv, dts)))
            if n == 0:
                ops.append((at_("prep"), functools.partial(prepare, first)))
            if last:
                ops.append((at_("step"), functools.partial(last_stats, n, first)))
                ops.append((at_("fin"), functools.partial(finish, n, first)))
            else:
                ops.append((at_("step"), functools.partial(pass_on, n, first, swapped)))
                if swapped:
                    ops.append((at_("swap"), functools.partial(swap_on, n)))
        if cross:
            feed(kk, FEED, mine_of(kk))
        greet()
        if not last:
            for dev in plane(k + 1):
                send(lgain_ref, lng.at[me], small_send.at[1], gain_sem.at[1], dev)
                send(lshift_ref, lnb.at[me], small_send.at[1], gain_sem.at[2], dev)
        for _, op in sorted(ops, key=lambda op: op[0]):
            op()
        drain(counts[0], relay_send.at[0])
        total = sg.shape[1]
        await_bytes(gains.at[pl.ds(0, G - 1)], small_send.at[0])
        if last:
            await_bytes(sfin.at[:, pl.ds(0, G - 1)], stat_send.at[0])
            if P_ > 1:
                drain(total - own_rows, back_send.at[0])
        else:
            await_bytes(sin.at[:, pl.ds(0, G)], stat_send.at[0])
            await_bytes(lng.at[pl.ds(0, G)], small_send.at[1])
            await_bytes(lnb.at[pl.ds(0, G)], small_send.at[1])
            drain(total * (T - len(zrelay)), next_send.at[0])
            if cross and F > 1:
                drain(2 * sum(c[1] for c in chunks if c[0] >= SWAP), swap_send.at[0])
            if not first:
                drain(total * T, next_send.at[0])

    if not cross:
        for q in range(feeds):
            feed(q, range(1, T), mine)
            if P_ > 1:
                pl.when(k != q)(functools.partial(feed, q, [0], mine))
    if P_ == 1:
        run(True, True)
    else:
        pl.when(k == 0)(lambda: run(True, False))
        pl.when(k == P_ - 1)(lambda: run(False, True))
        if P_ > 2:
            pl.when((k > 0) & (k < P_ - 1))(lambda: run(False, False))

    drain(own_rows * (T - 1 if cross else feeds * T - 1), feed_send.at[0])
    if P_ > 2:
        pl.when(k >= feeds)(lambda: await_bytes(x_ref, feed_send.at[0]))
    if P_ > 1:
        pl.when(k < P_ - 1)(lambda: await_bytes(out_ref, out_sem.at[0]))


def plan(sizes, own_rows):
    if sizes[0] == 2 and sizes[2] & (sizes[2] - 1) == 0 and all(sum(split) == own_rows for split in SPLITS):
        rows = [size for split in SPLITS for size in split]
        return [(sum(rows[:i]), size) for i, size in enumerate(rows)], True
    size = min(64, own_rows)
    return [(i * size, size) for i in range(own_rows * sizes[0] // size)], False


def when(chunks, own_rows, cross, kk, n, op):
    if cross and TIMES:
        return TIMES[kk][op][n] if op != "prep" else TIMES[kk]["step"][0] - 0.01
    start, size = chunks[n]
    late = start + size
    mine = late - start // own_rows * own_rows if cross else late
    own = not cross or start // own_rows == kk
    base = 6.6 + 1.4 * late / 64
    s0 = 3 + 0.7 * mine / 64 if own else 5.5 + 0.7 * mine / 64
    s1 = 5.5 + 1.4 * mine / 64 if own else 11.5 + 0.8 * mine / 64
    first = {"S0": s0, "S1": s1, "S2": s1 + 1, "step": s1 + 1.1, "prep": s1 + 1.05, "swap": s1 + 4, "fin": s1 + 6}
    later = {
        "S0": s0, "S1": s1, "C00": base + 3, "ent": base + 6, "ent2": base + 8, "C1": base + 9, "C2": base + 10,
        "prep": base + 5.9, "step": base + 10.1, "swap": base + 13, "fin": base + 15,
    }
    return (later if kk else first)[op]


def local(sizes, inputs, norm_gain, w_value, w_gate, w_taps, ln_gain, ln_shift):
    P_, F, T = sizes
    G = F * T
    own_rows, C = inputs.shape
    TOK = own_rows * P_
    chunks, _ = plan(sizes, own_rows)
    NC = len(chunks)
    D = w_value.shape[1]
    W = w_taps.shape[1]
    head = -(-(W - 1) // 8) * 8
    operands = (inputs, norm_gain, w_value, w_gate, w_taps, ln_gain, ln_shift)
    dma = pltpu.SemaphoreType.DMA
    f32, bf16 = jnp.float32, jnp.bfloat16
    V = pltpu.VMEM
    return pl.pallas_call(
        functools.partial(kernel, sizes),
        out_shape=pltpu.VMEM((own_rows, C), bf16),
        in_specs=[pl.BlockSpec(memory_space=pl.ANY)] * 7,
        out_specs=pl.BlockSpec(memory_space=pltpu.VMEM),
        scratch_shapes=[
            V(inputs.shape, bf16), V(norm_gain.shape, bf16), V((D, 2 * C), bf16), V(w_taps.shape, bf16),
            V(ln_gain.shape, f32), V(ln_shift.shape, f32),
            dma((len(operands),)),
            V((G, TOK, C), bf16), V((G, TOK, C), bf16), V((G, TOK, C), bf16),
            V((G, 1, C), f32), V((G, 1, C), f32), V((G, 1, C), f32),
            V((NC, G, 2, LEN), f32), V((NC, G, 2, LEN), f32), V((NC, 2, LEN), f32),
            V((LEN + head, C), f32), V((W, C), f32),
            V((TOK, C), f32), V((TOK, C), bf16), V((2, LEN, C), f32), V((TOK, C), bf16),
            V((LEN, LEN), f32),
            dma((NC, G)), dma((NC, G)), dma((NC, G)), dma((NC,)), dma((NC,)), dma((3,)), dma((1,)),
            dma((1,)), dma((1,)), dma((2,)), dma((1,)), dma((1,)), dma((1,)),
            V((TOK, C), bf16), dma((NC,)), dma((1,)),
        ],
        compiler_params=pltpu.CompilerParams(collective_id=0, has_side_effects=True),
    )(*operands)


def solution(mesh):
    sizes = (mesh.shape["pp"], mesh.shape["fs"], mesh.shape["tp"])
    in_specs = (
        P("pp", ("fs", "tp")),
        P("pp", ("fs", "tp")),
        P("pp", None, ("fs", "tp")),
        P("pp", None, ("fs", "tp")),
        P("pp", None, ("fs", "tp")),
        P("pp", ("fs", "tp")),
        P("pp", ("fs", "tp")),
    )
    out_specs = P("pp", ("fs", "tp"))
    return jax.shard_map(
        functools.partial(local, sizes), mesh=mesh, in_specs=in_specs, out_specs=out_specs,
        check_vma=False,
    )
```

```python
import functools

import jax
import jax.numpy as jnp
from jax import lax
from jax.experimental import pallas as pl
from jax.experimental.pallas import tpu as pltpu
from jax.sharding import PartitionSpec as P

LEN = 128
SPLITS = ((128, 128), (128, 128))
FEED = (2, 3, 1)
SEND = (0, 3, 2, 1)
ENTER = (0, 1, 3, 2)
XCARRY = (1, 2, 3)
ZRELAY = (1, 2)
SWAP = 256
TIMES = (
    {"S0": (-0.48, 4.35, 10.17, 11.39), "S1": (6.67, 11.13, 17.25, 20.33), "S2": (8.5, 15.39, 18.61, 20.55), "step": (8.5, 15.39, 18.61, 20.55), "swap": (0, 0, 31.88, 26.88)},
    {"S0": (10.67, 16.26, 7.57, 7.57), "C00": (16.08, 17.31, 18.47, 19.95), "ent": (18.0, 19.3, 21.72, 24.23), "C1": (21.04, 25.35, 26.83, 31.69), "C2": (21.81, 26.26, 31.37, 33.41), "step": (21.81, 26.27, 31.37, 33.42), "fin": (32.83, 34.11, 38.98, 44.31), "S1": (0, 0, 8.63, 11.78), "ent2": (0, 0, 29.86, 28.1)},
)


norm_eps = 1e-06
layer_eps = 1e-05
MESH = pl.DeviceIdType.MESH


def kernel(
    sizes,
    x_hbm,
    gain_hbm,
    wv_hbm,
    wg_hbm,
    taps_hbm,
    lgain_hbm,
    lshift_hbm,
    out_ref,
    x_ref,
    gain_ref,
    wcat,
    taps_ref,
    lgain_ref,
    lshift_ref,
    load_sem,
    sg,
    cg,
    hg,
    gains,
    lng,
    lnb,
    sin,
    sfin,
    sout,
    pad,
    taps,
    conv_own,
    conv_out,
    keep,
    new_buf,
    turn,
    s_sem,
    c_sem,
    h_sem,
    sin_sem,
    sfin_sem,
    gain_sem,
    out_sem,
    feed_send,
    relay_send,
    small_send,
    stat_send,
    next_send,
    back_send,
    side,
    side_sem,
    swap_send,
    meet_sem,
):
    P_, F, T = sizes
    G = F * T
    k, f, t = lax.axis_index("pp"), lax.axis_index("fs"), lax.axis_index("tp")
    C = conv_own.shape[1]
    D = wcat.shape[0]
    W = taps.shape[0]
    own_rows = x_ref.shape[0]
    head = pad.shape[0] - LEN
    me = f * T + t
    feeds = min(2, P_)

    loads = [
        pltpu.make_async_copy(a, b, load_sem.at[n])
        for n, (a, b) in enumerate(
            [
                (x_hbm, x_ref), (gain_hbm, gain_ref), (lgain_hbm, lgain_ref), (lshift_hbm, lshift_ref),
                (taps_hbm, taps_ref),
                (wv_hbm.at[0], wcat.at[:, pl.ds(0, C)]), (wg_hbm.at[0], wcat.at[:, pl.ds(C, C)]),
            ]
        )
    ]
    for load in loads:
        load.start()

    if T & (T - 1) == 0:
        to_t = [t] + [t ^ d for d in range(1, T)]
        from_t = to_t
    else:
        to_t = [lax.rem(t + d, T) for d in range(T)]
        from_t = [lax.rem(t + T - d, T) for d in range(T)]

    def at(kk, ff, tt):
        return {"pp": kk, "fs": ff, "tp": tt}

    def send(src, dst, s_sem_, r_sem, dev):
        pltpu.make_async_remote_copy(
            src_ref=src, dst_ref=dst, send_sem=s_sem_, recv_sem=r_sem, device_id=dev, device_id_type=MESH
        ).start()

    def await_bytes(ref, sem):
        pltpu.make_async_copy(ref, ref, sem).wait()

    peers = [at(k, lax.rem(f + df, F), to_t[dt]) for dt in range(T - 1, -1, -1) for df in range(F) if df or dt]

    def plane(kk):
        return [at(kk, lax.rem(f + df, F), to_t[dt]) for dt in range(T - 1, -1, -1) for df in range(F)]

    bits = []
    b = F // 2
    while b:
        bits.append(b)
        b //= 2
    pow2 = T & (T - 1) == 0
    every = tuple(range(T))
    chunks, cross = plan(sizes, own_rows)
    NCH = len(chunks)
    zrelay = ZRELAY if pow2 and T == 4 else ()

    def rows_of(n):
        return pl.ds(chunks[n][0], chunks[n][1])

    def feed(q, dts, mine):
        for n, start, i in mine:
            size = chunks[n][1] if cross else chunks[0][1]
            for dt in dts:
                send(
                    x_ref.at[pl.ds(i, size)], sg.at[me, pl.ds(start, size)], feed_send.at[0], s_sem.at[n, me],
                    at(q, f, to_t[dt]),
                )

    def own_copies(mine):
        for n, start, i in mine:
            size = chunks[n][1] if cross else chunks[0][1]
            pltpu.make_async_copy(
                x_hbm.at[pl.ds(i, size)], sg.at[me, pl.ds(start, size)], s_sem.at[n, me]
            ).start()

    def mine_of(kk):
        return [(n, c, c % own_rows) for n, (c, _) in enumerate(chunks) if c // own_rows == kk]

    if cross:
        for kk in range(P_):
            pl.when(k == kk)(functools.partial(own_copies, mine_of(kk)))
    else:
        size = chunks[0][1]
        mine = [(k * (own_rows // size) + i, k * own_rows + i * size, i * size) for i in range(own_rows // size)]
        if P_ > feeds:
            pl.when(k < feeds)(functools.partial(own_copies, mine))
        else:
            own_copies(mine)
    barrier = pltpu.get_barrier_semaphore()
    column = [at(k, f, tt) for tt in to_t[1:]]
    if cross:
        everyone = column + [at(k, f ^ b, t) for b in bits] + [at(1 - k, f, t)]
    else:
        everyone = peers + [dev for dk in range(1, P_) for dev in plane(lax.rem(k + dk, P_))]
    for dev in everyone:
        pl.semaphore_signal(barrier, inc=1, device_id=dev, device_id_type=MESH)
    for load in loads[:4]:
        load.wait()
    gains[me] = gain_ref[...].astype(jnp.float32)
    lgain_ref[...] = lgain_ref[...] * 0.5
    lshift_ref[...] = lshift_ref[...] * 0.5
    pad[0:head, :] = jnp.zeros((head, C), jnp.float32)
    turn[...] = jnp.zeros_like(turn)
    pl.semaphore_wait(barrier, len(everyone))

    def meet():
        for i, b in enumerate(bits):
            pl.semaphore_signal(meet_sem.at[i], inc=1, device_id=at(k, f ^ b, t), device_id_type=MESH)
            pl.semaphore_wait(meet_sem.at[i], 1)
        pl.semaphore_signal(meet_sem.at[top], inc=1, device_id=at(1 - k, f, t), device_id_type=MESH)

    def give(n, i, start, size, dev):
        send(x_ref.at[pl.ds(i, size)], sg.at[me, pl.ds(start, size)], relay_send.at[0], s_sem.at[n, me], dev)
        counts[0] += size

    def greet():
        for dev in peers:
            send(gains.at[me], gains.at[me], small_send.at[0], gain_sem.at[0], dev)

    top = len(bits)
    counts = [0]

    def forward(buf, sem, n, slot, dev):
        block = buf.at[slot, rows_of(n)]
        send(block, block, relay_send.at[0], sem.at[n, slot], dev)
        counts[0] += chunks[n][1]

    def arrived(buf, sem, n, slot):
        await_bytes(buf.at[slot, rows_of(n)], sem.at[n, slot])

    def stage(r):
        return 0 if r == 0 else len(bits) - ((r & -r).bit_length() - 1)

    def hop(buf, sem, n, lv, dts, ups=every, down=True, over=(), given=False):
        for r in range(F):
            if stage(r) != lv:
                continue
            for dt in dts:
                slot = (f ^ r) * T + from_t[dt]
                arrived(buf, sem, n, slot)
                if given and dt == 0:
                    continue
                for b in bits:
                    if b < ((r & -r) or F) and (dt in ups if b == F // 2 else down):
                        forward(buf, sem, n, slot, at(k, f ^ b, t))
                if dt in over:
                    forward(buf, sem, n, slot, at(1 - k, f, t))

    def prepare(first):
        if not first:
            await_bytes(lng.at[pl.ds(0, G)], gain_sem.at[1])
            await_bytes(lnb.at[pl.ds(0, G)], gain_sem.at[2])
        for load in loads[4:]:
            load.wait()
        taps[...] = taps_ref[0].astype(jnp.float32)
        await_bytes(gains.at[pl.ds(0, G - 1)], gain_sem.at[0])
        for s in range(G):
            turn[s : s + 1, :] = gains[s]
        cols = turn[...].T
        for s in range(G):
            rows = pl.ds(s * C, C)
            wcat[rows, :] = (wcat[rows, :].astype(jnp.float32) * cols[:, s : s + 1]).astype(jnp.bfloat16)

    def moments(ref, n):
        R = chunks[n][1]
        turn[0:2, :] = jnp.sum(ref[n], axis=0)
        cols = turn[...].T
        mu = cols[0:R, 0:1] / D
        var = cols[0:R, 1:2] / D - mu * mu
        return mu, lax.rsqrt(var + layer_eps)

    def layer_end(n, slot, mu, rs):
        half = (cg[slot, rows_of(n)].astype(jnp.float32) - mu) * rs * lng[slot] + lnb[slot]
        hg[slot, rows_of(n)] = (
            sg[slot, rows_of(n)].astype(jnp.float32) + (half + half * jnp.tanh(half))
        ).astype(jnp.bfloat16)

    def enter(n, swapped):
        await_bytes(sin.at[n, pl.ds(0, G)], sin_sem.at[n])
        mu, rs = moments(sin, n)
        if swapped:
            keep[n, 0, 0 : chunks[n][1], :] = jnp.broadcast_to(mu, (chunks[n][1], C))
            keep[n, 1, 0 : chunks[n][1], :] = jnp.broadcast_to(rs, (chunks[n][1], C))
        for dt in (ENTER if len(ENTER) == T else every):
            slot = f * T + from_t[dt]
            if dt or not zrelay:
                arrived(cg, c_sem, n, slot)
            layer_end(n, slot, mu, rs)
            for b in bits:
                if not (swapped and dt == 0 and b == F // 2):
                    forward(hg, h_sem, n, slot, at(k, f ^ b, t))

    def enter_swapped(n):
        slot = (f ^ (F // 2)) * T + t
        arrived(cg, c_sem, n, slot)
        layer_end(n, slot, keep[n, 0, 0 : chunks[n][1], :], keep[n, 1, 0 : chunks[n][1], :])
        for b in bits[1:]:
            forward(hg, h_sem, n, slot, at(k, f ^ b, t))

    def spread(n):
        slot = f * T + t
        arrived(cg, c_sem, n, slot)
        for dz in zrelay:
            forward(cg, c_sem, n, slot, at(k, f, to_t[dz]))

    def project(n, buf):
        start, R = chunks[n]
        blocks = [buf[s, rows_of(n)] for s in range(G)]
        squares = jnp.zeros((R, C), jnp.float32)
        for xb in blocks:
            xf = xb.astype(jnp.float32)
            squares = squares + xf * xf
        scale = lax.rsqrt(jnp.sum(squares, axis=1, keepdims=True) / D + norm_eps)
        both = jnp.dot(jnp.concatenate(blocks, axis=1), wcat[...], preferred_element_type=jnp.float32) * scale
        j = start % LEN
        pad[head + j : head + j + R, :] = both[:, :C] * (0.5 + 0.5 * jnp.tanh(0.5 * both[:, C:]))
        step = 32 if R % 32 == 0 else R
        for r0 in range(0, R, step):
            acc = jnp.zeros((step, C), jnp.float32)
            for w in range(W):
                o = head - (W - 1) + w + j + r0
                acc = acc + pad[o : o + step, :] * taps[w : w + 1, :]
            conv_own[start + r0 : start + r0 + step, :] = acc
        conv = conv_own[start : start + R, :]
        lane = lax.broadcasted_iota(jnp.int32, (R, LEN), 1)
        s1 = jnp.sum(conv, axis=1, keepdims=True)
        s2 = jnp.sum(conv * conv, axis=1, keepdims=True)
        turn[0:R, :] = jnp.where(lane == 0, s1, jnp.where(lane == 1, s2, 0.0))
        return conv, turn[...].T[0:2, :]

    def pass_on(n, first, swapped):
        conv, stat = project(n, sg if first else hg)
        rows = rows_of(n)
        sout[n] = stat
        conv_out[rows, :] = conv.astype(jnp.bfloat16)
        for dev in plane(k + 1):
            send(sout.at[n], sin.at[n, me], stat_send.at[0], sin_sem.at[n], dev)
        for dt in SEND if len(SEND) == T else every:
            if dt not in zrelay:
                send(conv_out.at[rows], cg.at[me, rows], next_send.at[0], c_sem.at[n, me], at(k + 1, f, to_t[dt]))
        if swapped:
            send(conv_out.at[rows], side.at[rows], swap_send.at[0], side_sem.at[n], at(k, f ^ (F // 2), t))
        if not first:
            for tt in to_t:
                send(hg.at[me, rows], sg.at[me, rows], next_send.at[0], s_sem.at[n, me], at(k + 1, f, tt))

    def swap_on(n):
        rows = rows_of(n)
        await_bytes(side.at[rows], side_sem.at[n])
        slot = (f ^ (F // 2)) * T + t
        send(side.at[rows], cg.at[slot, rows], swap_send.at[0], c_sem.at[n, slot], at(k + 1, f, t))

    def last_stats(n, first):
        _, stat = project(n, sg if first else hg)
        sfin[n, me] = stat
        for dev in peers:
            send(sfin.at[n, me], sfin.at[n, me], stat_send.at[0], sfin_sem.at[n], dev)

    def finish(n, first):
        start, R = chunks[n]
        await_bytes(sfin.at[n, pl.ds(0, G - 1)], sfin_sem.at[n])
        mu, rs = moments(sfin, n)
        half = (conv_own[start : start + R, :] - mu) * rs * lgain_ref[...] + lshift_ref[...]
        stream = (sg if first else hg)[me, rows_of(n)]
        new = (stream.astype(jnp.float32) + (half + half * jnp.tanh(half))).astype(jnp.bfloat16)
        owner, i = start // own_rows, start % own_rows
        rows = pl.ds(i, R)
        if owner == P_ - 1:
            out_ref[rows, :] = new
        else:
            new_buf[rows_of(n), :] = new
            send(new_buf.at[rows_of(n)], out_ref.at[rows], back_send.at[0], out_sem.at[0], at(owner, f, t))

    def drain(rows, sem):
        full = sg.shape[1]
        while rows >= full:
            m = min(G, rows // full)
            await_bytes(sg.at[pl.ds(0, m)], sem)
            rows -= m * full
        if rows:
            await_bytes(sg.at[0, pl.ds(0, rows)], sem)

    def run(first, last):
        counts[0] = 0
        kk = 0 if first else 1
        ops = []
        for n, (start, size) in enumerate(chunks):
            own = not cross or start // own_rows == kk
            swapped = cross and F > 1 and start >= SWAP
            at_ = functools.partial(when, chunks, own_rows, cross, kk, n)
            x1 = XCARRY if cross else ()
            zero = (0,) if swapped else ()
            if first:
                if own:
                    ops.append((at_("S0"), functools.partial(hop, sg, s_sem, n, 0, every, over=every if cross else (), given=cross)))
                else:
                    ups = tuple(d for d in every if d not in x1)
                    ops.append((at_("S0"), functools.partial(hop, sg, s_sem, n, 0, every, ups)))
                for lv in range(1, top + 1):
                    over = zero if own and lv == 1 else ()
                    ops.append((at_("S%d" % min(lv, 2)), functools.partial(hop, sg, s_sem, n, lv, every, over=over)))
            else:
                if cross and own:
                    ups = tuple(sorted(set(x1 + zero)))
                    ops.append((at_("S0"), functools.partial(hop, sg, s_sem, n, 0, every, ups, False, every, True)))
                    if ups:
                        ops.append((at_("S1"), functools.partial(hop, sg, s_sem, n, 1, ups, (), False, x1)))
                else:
                    ops.append((at_("S0"), functools.partial(hop, sg, s_sem, n, 0, every, (), False)))
                    if swapped:
                        ops.append((at_("S1"), functools.partial(hop, sg, s_sem, n, 1, (0,), (), False)))
                if zrelay:
                    ops.append((at_("C00"), functools.partial(spread, n)))
                ops.append((at_("ent"), functools.partial(enter, n, swapped)))
                if swapped:
                    ops.append((at_("ent2"), functools.partial(enter_swapped, n)))
                for lv in range(1, top + 1):
                    dts = every[1:] if swapped and lv == 1 else every
                    ops.append((at_("C%d" % min(lv, 2)), functools.partial(hop, hg, h_sem, n, lv, dts)))
            if n == 0:
                ops.append((at_("prep"), functools.partial(prepare, first)))
            if last:
                ops.append((at_("step"), functools.partial(last_stats, n, first)))
                ops.append((at_("fin"), functools.partial(finish, n, first)))
            else:
                ops.append((at_("step"), functools.partial(pass_on, n, first, swapped)))
                if swapped:
                    ops.append((at_("swap"), functools.partial(swap_on, n)))
        if cross:
            for entry in mine_of(kk):
                feed(kk, FEED, [entry])
                n, start, i = entry
                size = chunks[n][1]
                swapped = start >= SWAP
                for b in bits:
                    if (first or 0 in XCARRY or swapped) if b == F // 2 else first:
                        give(n, i, start, size, at(k, f ^ b, t))
                give(n, i, start, size, at(1 - k, f, t))
            meet()
        greet()
        if cross:
            pl.semaphore_wait(meet_sem.at[top], 1)
        if not last:
            for dev in plane(k + 1):
                send(lgain_ref, lng.at[me], small_send.at[1], gain_sem.at[1], dev)
                send(lshift_ref, lnb.at[me], small_send.at[1], gain_sem.at[2], dev)
        for _, op in sorted(ops, key=lambda op: op[0]):
            op()
        drain(counts[0], relay_send.at[0])
        total = sg.shape[1]
        await_bytes(gains.at[pl.ds(0, G - 1)], small_send.at[0])
        if last:
            await_bytes(sfin.at[:, pl.ds(0, G - 1)], stat_send.at[0])
            if P_ > 1:
                drain(total - own_rows, back_send.at[0])
        else:
            await_bytes(sin.at[:, pl.ds(0, G)], stat_send.at[0])
            await_bytes(lng.at[pl.ds(0, G)], small_send.at[1])
            await_bytes(lnb.at[pl.ds(0, G)], small_send.at[1])
            drain(total * (T - len(zrelay)), next_send.at[0])
            if cross and F > 1:
                drain(2 * sum(c[1] for c in chunks if c[0] >= SWAP), swap_send.at[0])
            if not first:
                drain(total * T, next_send.at[0])

    if not cross:
        for q in range(feeds):
            feed(q, range(1, T), mine)
            if P_ > 1:
                pl.when(k != q)(functools.partial(feed, q, [0], mine))
    if P_ == 1:
        run(True, True)
    else:
        pl.when(k == 0)(lambda: run(True, False))
        pl.when(k == P_ - 1)(lambda: run(False, True))
        if P_ > 2:
            pl.when((k > 0) & (k < P_ - 1))(lambda: run(False, False))

    drain(own_rows * (T - 1 if cross else feeds * T - 1), feed_send.at[0])
    if P_ > 2:
        pl.when(k >= feeds)(lambda: await_bytes(x_ref, feed_send.at[0]))
    if P_ > 1:
        pl.when(k < P_ - 1)(lambda: await_bytes(out_ref, out_sem.at[0]))


def plan(sizes, own_rows):
    if sizes[0] == 2 and sizes[2] & (sizes[2] - 1) == 0 and all(sum(split) == own_rows for split in SPLITS):
        rows = [size for split in SPLITS for size in split]
        return [(sum(rows[:i]), size) for i, size in enumerate(rows)], True
    size = min(64, own_rows)
    return [(i * size, size) for i in range(own_rows * sizes[0] // size)], False


def when(chunks, own_rows, cross, kk, n, op):
    if cross and TIMES:
        if op == "prep":
            return TIMES[kk]["C00" if kk else "step"][0] - 0.01
        return TIMES[kk][op][n]
    start, size = chunks[n]
    late = start + size
    mine = late - start // own_rows * own_rows if cross else late
    own = not cross or start // own_rows == kk
    base = 6.6 + 1.4 * late / 64
    s0 = 3 + 0.7 * mine / 64 if own else 5.5 + 0.7 * mine / 64
    s1 = 5.5 + 1.4 * mine / 64 if own else 11.5 + 0.8 * mine / 64
    first = {"S0": s0, "S1": s1, "S2": s1 + 1, "step": s1 + 1.1, "prep": s1 + 1.05, "swap": s1 + 4, "fin": s1 + 6}
    later = {
        "S0": s0, "S1": s1, "C00": base + 3, "ent": base + 6, "ent2": base + 8, "C1": base + 9, "C2": base + 10,
        "prep": base + 2.9, "step": base + 10.1, "swap": base + 13, "fin": base + 15,
    }
    return (later if kk else first)[op]


def local(sizes, inputs, norm_gain, w_value, w_gate, w_taps, ln_gain, ln_shift):
    P_, F, T = sizes
    G = F * T
    own_rows, C = inputs.shape
    TOK = own_rows * P_
    chunks, _ = plan(sizes, own_rows)
    NC = len(chunks)
    D = w_value.shape[1]
    W = w_taps.shape[1]
    head = -(-(W - 1) // 8) * 8
    operands = (inputs, norm_gain, w_value, w_gate, w_taps, ln_gain, ln_shift)
    dma = pltpu.SemaphoreType.DMA
    f32, bf16 = jnp.float32, jnp.bfloat16
    V = pltpu.VMEM
    return pl.pallas_call(
        functools.partial(kernel, sizes),
        out_shape=pltpu.VMEM((own_rows, C), bf16),
        in_specs=[pl.BlockSpec(memory_space=pl.ANY)] * 7,
        out_specs=pl.BlockSpec(memory_space=pltpu.VMEM),
        scratch_shapes=[
            V(inputs.shape, bf16), V(norm_gain.shape, bf16), V((D, 2 * C), bf16), V(w_taps.shape, bf16),
            V(ln_gain.shape, f32), V(ln_shift.shape, f32),
            dma((len(operands),)),
            V((G, TOK, C), bf16), V((G, TOK, C), bf16), V((G, TOK, C), bf16),
            V((G, 1, C), f32), V((G, 1, C), f32), V((G, 1, C), f32),
            V((NC, G, 2, LEN), f32), V((NC, G, 2, LEN), f32), V((NC, 2, LEN), f32),
            V((LEN + head, C), f32), V((W, C), f32),
            V((TOK, C), f32), V((TOK, C), bf16), V((NC, 2, LEN, C), f32), V((TOK, C), bf16),
            V((LEN, LEN), f32),
            dma((NC, G)), dma((NC, G)), dma((NC, G)), dma((NC,)), dma((NC,)), dma((3,)), dma((1,)),
            dma((1,)), dma((1,)), dma((2,)), dma((1,)), dma((1,)), dma((1,)),
            V((TOK, C), bf16), dma((NC,)), dma((1,)), pltpu.SemaphoreType.REGULAR((8,)),
        ],
        compiler_params=pltpu.CompilerParams(collective_id=0, has_side_effects=True),
    )(*operands)


def solution(mesh):
    sizes = (mesh.shape["pp"], mesh.shape["fs"], mesh.shape["tp"])
    in_specs = (
        P("pp", ("fs", "tp")),
        P("pp", ("fs", "tp")),
        P("pp", None, ("fs", "tp")),
        P("pp", None, ("fs", "tp")),
        P("pp", None, ("fs", "tp")),
        P("pp", ("fs", "tp")),
        P("pp", ("fs", "tp")),
    )
    out_specs = P("pp", ("fs", "tp"))
    return jax.shard_map(
        functools.partial(local, sizes), mesh=mesh, in_specs=in_specs, out_specs=out_specs,
        check_vma=False,
    )
```

```python
import functools

import jax
import jax.numpy as jnp
from jax import lax
from jax.experimental import pallas as pl
from jax.experimental.pallas import tpu as pltpu
from jax.sharding import PartitionSpec as P

LEN = 128
SPLITS = ((128, 128), (128, 128))
FEED = (2, 3, 1)
SEND = (0, 3, 2, 1)
ENTER = (0, 1, 3, 2)
XCARRY = (1, 2, 3)
ZRELAY = (1, 2)
SWAP = 256
TIMES = (
    {"S0": (-0.48, 4.35, 10.17, 11.39), "S1": (6.67, 11.13, 17.25, 20.33), "S2": (8.5, 15.39, 18.61, 20.55), "step": (8.5, 15.39, 18.61, 20.55), "swap": (0, 0, 31.88, 26.88)},
    {"S0": (10.67, 16.26, 7.57, 7.57), "C00": (16.08, 17.31, 18.47, 19.95), "ent": (18.0, 19.3, 21.72, 24.23), "C1": (21.04, 25.35, 26.83, 31.69), "C2": (21.81, 26.26, 31.37, 33.41), "step": (21.81, 26.27, 31.37, 33.42), "fin": (32.83, 34.11, 38.98, 44.31), "S1": (0, 0, 8.63, 11.78), "ent2": (0, 0, 29.86, 28.1)},
)


norm_eps = 1e-06
layer_eps = 1e-05
MESH = pl.DeviceIdType.MESH


def kernel(
    sizes,
    x_hbm,
    gain_hbm,
    wv_hbm,
    wg_hbm,
    taps_hbm,
    lgain_hbm,
    lshift_hbm,
    out_ref,
    x_ref,
    gain_ref,
    wcat,
    taps_ref,
    lgain_ref,
    lshift_ref,
    load_sem,
    sg,
    cg,
    hg,
    gains,
    lng,
    sin,
    sfin,
    sout,
    pad,
    taps,
    conv_own,
    conv_out,
    keep,
    lnp,
    new_buf,
    turn,
    s_sem,
    c_sem,
    h_sem,
    sin_sem,
    sfin_sem,
    gain_sem,
    out_sem,
    sent,
    side,
    side_sem,
    meet_sem,
):
    P_, F, T = sizes
    G = F * T
    k, f, t = lax.axis_index("pp"), lax.axis_index("fs"), lax.axis_index("tp")
    C = conv_own.shape[1]
    D = wcat.shape[0]
    W = taps.shape[0]
    own_rows = x_ref.shape[0]
    head = pad.shape[0] - LEN
    me = f * T + t
    feeds = min(2, P_)

    loads = [
        pltpu.make_async_copy(a, b, load_sem.at[n])
        for n, (a, b) in enumerate(
            [
                (x_hbm, x_ref), (gain_hbm, gain_ref), (lgain_hbm, lgain_ref), (lshift_hbm, lshift_ref),
                (taps_hbm, taps_ref),
                (wv_hbm.at[0], wcat.at[:, pl.ds(0, C)]), (wg_hbm.at[0], wcat.at[:, pl.ds(C, C)]),
            ]
        )
    ]
    for load in loads:
        load.start()

    if T & (T - 1) == 0:
        to_t = [t] + [t ^ d for d in range(1, T)]
        from_t = to_t
    else:
        to_t = [lax.rem(t + d, T) for d in range(T)]
        from_t = [lax.rem(t + T - d, T) for d in range(T)]

    def at(kk, ff, tt):
        return {"pp": kk, "fs": ff, "tp": tt}

    def send(src, dst, s_sem_, r_sem, dev):
        pltpu.make_async_remote_copy(
            src_ref=src, dst_ref=dst, send_sem=s_sem_, recv_sem=r_sem, device_id=dev, device_id_type=MESH
        ).start()

    def await_bytes(ref, sem):
        pltpu.make_async_copy(ref, ref, sem).wait()

    peers = [at(k, lax.rem(f + df, F), to_t[dt]) for dt in range(T - 1, -1, -1) for df in range(F) if df or dt]

    def plane(kk):
        return [at(kk, lax.rem(f + df, F), to_t[dt]) for dt in range(T - 1, -1, -1) for df in range(F)]

    bits = []
    b = F // 2
    while b:
        bits.append(b)
        b //= 2
    pow2 = T & (T - 1) == 0
    every = tuple(range(T))
    chunks, cross = plan(sizes, own_rows)
    NCH = len(chunks)
    zrelay = ZRELAY if pow2 and T == 4 else ()

    def rows_of(n):
        return pl.ds(chunks[n][0], chunks[n][1])

    def feed(q, dts, mine):
        for n, start, i in mine:
            size = chunks[n][1] if cross else chunks[0][1]
            for dt in dts:
                send(
                    x_ref.at[pl.ds(i, size)], sg.at[me, pl.ds(start, size)], sent.at[0], s_sem.at[n, dt],
                    at(q, f, to_t[dt]),
                )

    def own_copies(mine):
        for n, start, i in mine:
            size = chunks[n][1] if cross else chunks[0][1]
            pltpu.make_async_copy(
                x_hbm.at[pl.ds(i, size)], sg.at[me, pl.ds(start, size)], s_sem.at[n, 0]
            ).start()

    def mine_of(kk):
        return [(n, c, c % own_rows) for n, (c, _) in enumerate(chunks) if c // own_rows == kk]

    if cross:
        for kk in range(P_):
            pl.when(k == kk)(functools.partial(own_copies, mine_of(kk)))
    else:
        size = chunks[0][1]
        mine = [(k * (own_rows // size) + i, k * own_rows + i * size, i * size) for i in range(own_rows // size)]
        if P_ > feeds:
            pl.when(k < feeds)(functools.partial(own_copies, mine))
        else:
            own_copies(mine)
    barrier = pltpu.get_barrier_semaphore()
    column = [at(k, f, tt) for tt in to_t[1:]]
    if cross:
        everyone = column + [at(k, f ^ b, t) for b in bits] + [at(1 - k, f, t)]
    else:
        everyone = peers + [dev for dk in range(1, P_) for dev in plane(lax.rem(k + dk, P_))]
    for dev in everyone:
        pl.semaphore_signal(barrier, inc=1, device_id=dev, device_id_type=MESH)
    for load in loads[:4]:
        load.wait()
    gains[me] = gain_ref[...].astype(jnp.float32)
    lnp[0] = lgain_ref[...] * 0.5
    lnp[1] = lshift_ref[...] * 0.5
    pad[0:head, :] = jnp.zeros((head, C), jnp.float32)
    turn[...] = jnp.zeros_like(turn)
    pl.semaphore_wait(barrier, len(everyone))

    def meet():
        for i, b in enumerate(bits):
            pl.semaphore_signal(meet_sem.at[i], inc=1, device_id=at(k, f ^ b, t), device_id_type=MESH)
            pl.semaphore_wait(meet_sem.at[i], 1)
        pl.semaphore_signal(meet_sem.at[top], inc=1, device_id=at(1 - k, f, t), device_id_type=MESH)

    def give(n, i, start, size, cls, dev):
        send(x_ref.at[pl.ds(i, size)], sg.at[me, pl.ds(start, size)], sent.at[0], s_sem.at[n, cls], dev)
        counts[0] += size

    def greet():
        for dev in peers:
            send(gains.at[me], gains.at[me], sent.at[0], gain_sem.at[0], dev)

    top = len(bits)
    counts = [0]

    def stage(r):
        return 0 if r == 0 else len(bits) - ((r & -r).bit_length() - 1)

    relayed = [r for r in range(F) if not top or stage(r) < top]
    ends = [r for r in range(F) if r not in relayed]

    def kind(r, dt):
        if top and stage(r) == top:
            return len(relayed) * T
        return relayed.index(r) * T + dt

    def forward(buf, sem, n, slot, cls, dev):
        block = buf.at[slot, rows_of(n)]
        send(block, block, sent.at[0], sem.at[n, cls], dev)
        counts[0] += chunks[n][1]

    def arrived(buf, sem, n, slot, cls):
        await_bytes(buf.at[slot, rows_of(n)], sem.at[n, cls])

    def hop(buf, sem, n, lv, dts, ups=every, down=True, over=(), given=False, base=0):
        if top and lv == top:
            await_bytes(buf.at[pl.ds(0, len(ends) * T), rows_of(n)], sem.at[n, kind(ends[0], 0) - base])
            return
        for r in range(F):
            if stage(r) != lv:
                continue
            for dt in dts:
                slot = (f ^ r) * T + from_t[dt]
                arrived(buf, sem, n, slot, kind(r, dt) - base)
                if given and dt == 0:
                    continue
                for b in bits:
                    if b < ((r & -r) or F) and (dt in ups if b == F // 2 else down):
                        forward(buf, sem, n, slot, kind(r ^ b, dt) - base, at(k, f ^ b, t))
                if dt in over:
                    forward(buf, sem, n, slot, kind(r, dt) - base, at(1 - k, f, t))

    def prepare(first):
        if not first:
            await_bytes(lng.at[pl.ds(0, G)], gain_sem.at[1])
        for load in loads[4:]:
            load.wait()
        taps[...] = taps_ref[0].astype(jnp.float32)
        await_bytes(gains.at[pl.ds(0, G - 1)], gain_sem.at[0])
        for s in range(G):
            turn[s : s + 1, :] = gains[s]
        cols = turn[...].T
        for s in range(G):
            rows = pl.ds(s * C, C)
            wcat[rows, :] = (wcat[rows, :].astype(jnp.float32) * cols[:, s : s + 1]).astype(jnp.bfloat16)

    def moments(ref, n):
        R = chunks[n][1]
        turn[0:2, :] = jnp.sum(ref[n], axis=0)
        cols = turn[...].T
        mu = cols[0:R, 0:1] / D
        var = cols[0:R, 1:2] / D - mu * mu
        return mu, lax.rsqrt(var + layer_eps)

    def layer_end(n, slot, mu, rs):
        half = (cg[slot, rows_of(n)].astype(jnp.float32) - mu) * rs * lng[slot, 0] + lng[slot, 1]
        hg[slot, rows_of(n)] = (
            sg[slot, rows_of(n)].astype(jnp.float32) + (half + half * jnp.tanh(half))
        ).astype(jnp.bfloat16)

    def enter(n, swapped):
        await_bytes(sin.at[n, pl.ds(0, G)], sin_sem.at[n])
        mu, rs = moments(sin, n)
        if swapped:
            keep[n, 0, 0 : chunks[n][1], :] = jnp.broadcast_to(mu, (chunks[n][1], C))
            keep[n, 1, 0 : chunks[n][1], :] = jnp.broadcast_to(rs, (chunks[n][1], C))
        for dt in (ENTER if len(ENTER) == T else every):
            slot = f * T + from_t[dt]
            if dt or not zrelay:
                arrived(cg, c_sem, n, slot, dt)
            layer_end(n, slot, mu, rs)
            for b in bits:
                if not (swapped and dt == 0 and b == F // 2):
                    forward(hg, h_sem, n, slot, kind(b, dt) - T, at(k, f ^ b, t))

    def enter_swapped(n):
        slot = (f ^ (F // 2)) * T + t
        arrived(cg, c_sem, n, slot, T)
        layer_end(n, slot, keep[n, 0, 0 : chunks[n][1], :], keep[n, 1, 0 : chunks[n][1], :])
        for b in bits[1:]:
            forward(hg, h_sem, n, slot, kind(F // 2 ^ b, 0) - T, at(k, f ^ b, t))

    def spread(n):
        slot = f * T + t
        arrived(cg, c_sem, n, slot, 0)
        for dz in zrelay:
            forward(cg, c_sem, n, slot, dz, at(k, f, to_t[dz]))

    def project(n, buf):
        start, R = chunks[n]
        blocks = [buf[s, rows_of(n)] for s in range(G)]
        squares = jnp.zeros((R, C), jnp.float32)
        for xb in blocks:
            xf = xb.astype(jnp.float32)
            squares = squares + xf * xf
        scale = lax.rsqrt(jnp.sum(squares, axis=1, keepdims=True) / D + norm_eps)
        both = jnp.dot(jnp.concatenate(blocks, axis=1), wcat[...], preferred_element_type=jnp.float32) * scale
        j = start % LEN
        pad[head + j : head + j + R, :] = both[:, :C] * (0.5 + 0.5 * jnp.tanh(0.5 * both[:, C:]))
        step = 32 if R % 32 == 0 else R
        for r0 in range(0, R, step):
            acc = jnp.zeros((step, C), jnp.float32)
            for w in range(W):
                o = head - (W - 1) + w + j + r0
                acc = acc + pad[o : o + step, :] * taps[w : w + 1, :]
            conv_own[start + r0 : start + r0 + step, :] = acc
        conv = conv_own[start : start + R, :]
        lane = lax.broadcasted_iota(jnp.int32, (R, LEN), 1)
        s1 = jnp.sum(conv, axis=1, keepdims=True)
        s2 = jnp.sum(conv * conv, axis=1, keepdims=True)
        turn[0:R, :] = jnp.where(lane == 0, s1, jnp.where(lane == 1, s2, 0.0))
        return conv, turn[...].T[0:2, :]

    def pass_on(n, first, swapped):
        conv, stat = project(n, sg if first else hg)
        rows = rows_of(n)
        sout[n] = stat
        conv_out[rows, :] = conv.astype(jnp.bfloat16)
        for dev in plane(k + 1):
            send(sout.at[n], sin.at[n, me], sent.at[0], sin_sem.at[n], dev)
        for dt in SEND if len(SEND) == T else every:
            if dt not in zrelay:
                send(conv_out.at[rows], cg.at[me, rows], sent.at[0], c_sem.at[n, dt], at(k + 1, f, to_t[dt]))
        if swapped:
            send(conv_out.at[rows], side.at[rows], sent.at[0], side_sem.at[n], at(k, f ^ (F // 2), t))
        if not first:
            for dt in every:
                send(hg.at[me, rows], sg.at[me, rows], sent.at[0], s_sem.at[n, dt], at(k + 1, f, to_t[dt]))

    def swap_on(n):
        rows = rows_of(n)
        await_bytes(side.at[rows], side_sem.at[n])
        slot = (f ^ (F // 2)) * T + t
        send(side.at[rows], cg.at[slot, rows], sent.at[0], c_sem.at[n, T], at(k + 1, f, t))

    def last_stats(n, first):
        _, stat = project(n, sg if first else hg)
        sfin[n, me] = stat
        for dev in peers:
            send(sfin.at[n, me], sfin.at[n, me], sent.at[0], sfin_sem.at[n], dev)

    def finish(n, first):
        start, R = chunks[n]
        await_bytes(sfin.at[n, pl.ds(0, G - 1)], sfin_sem.at[n])
        mu, rs = moments(sfin, n)
        half = (conv_own[start : start + R, :] - mu) * rs * lnp[0] + lnp[1]
        stream = (sg if first else hg)[me, rows_of(n)]
        new = (stream.astype(jnp.float32) + (half + half * jnp.tanh(half))).astype(jnp.bfloat16)
        owner, i = start // own_rows, start % own_rows
        rows = pl.ds(i, R)
        if owner == P_ - 1:
            out_ref[rows, :] = new
        else:
            new_buf[rows_of(n), :] = new
            send(new_buf.at[rows_of(n)], out_ref.at[rows], sent.at[0], out_sem.at[0], at(owner, f, t))

    def drain(rows, sem):
        full = sg.shape[1]
        while rows >= full:
            m = min(G, rows // full)
            await_bytes(sg.at[pl.ds(0, m)], sem)
            rows -= m * full
        if rows:
            await_bytes(sg.at[0, pl.ds(0, rows)], sem)

    def run(first, last):
        counts[0] = 0
        kk = 0 if first else 1
        ops = []
        for n, (start, size) in enumerate(chunks):
            own = not cross or start // own_rows == kk
            swapped = cross and F > 1 and start >= SWAP
            at_ = functools.partial(when, chunks, own_rows, cross, kk, n)
            x1 = XCARRY if cross else ()
            zero = (0,) if swapped else ()
            if first:
                if own:
                    ops.append((at_("S0"), functools.partial(hop, sg, s_sem, n, 0, every, over=every if cross else (), given=cross)))
                else:
                    ups = tuple(d for d in every if d not in x1)
                    ops.append((at_("S0"), functools.partial(hop, sg, s_sem, n, 0, every, ups)))
                for lv in range(1, top + 1):
                    over = zero if own and lv == 1 else ()
                    ops.append((at_("S%d" % min(lv, 2)), functools.partial(hop, sg, s_sem, n, lv, every, over=over)))
            else:
                if cross and own:
                    ups = tuple(sorted(set(x1 + zero)))
                    ops.append((at_("S0"), functools.partial(hop, sg, s_sem, n, 0, every, ups, False, every, True)))
                    if ups:
                        ops.append((at_("S1"), functools.partial(hop, sg, s_sem, n, 1, ups, (), False, x1)))
                else:
                    ops.append((at_("S0"), functools.partial(hop, sg, s_sem, n, 0, every, (), False)))
                    if swapped:
                        ops.append((at_("S1"), functools.partial(hop, sg, s_sem, n, 1, (0,), (), False)))
                if zrelay:
                    ops.append((at_("C00"), functools.partial(spread, n)))
                ops.append((at_("ent"), functools.partial(enter, n, swapped)))
                if swapped:
                    ops.append((at_("ent2"), functools.partial(enter_swapped, n)))
                for lv in range(1, top + 1):
                    dts = every[1:] if swapped and lv == 1 else every
                    ops.append((at_("C%d" % min(lv, 2)), functools.partial(hop, hg, h_sem, n, lv, dts, base=T)))
            if n == 0:
                ops.append((at_("prep"), functools.partial(prepare, first)))
            if last:
                ops.append((at_("step"), functools.partial(last_stats, n, first)))
                ops.append((at_("fin"), functools.partial(finish, n, first)))
            else:
                ops.append((at_("step"), functools.partial(pass_on, n, first, swapped)))
                if swapped:
                    ops.append((at_("swap"), functools.partial(swap_on, n)))
        if cross:
            for entry in mine_of(kk):
                feed(kk, FEED, [entry])
                n, start, i = entry
                size = chunks[n][1]
                swapped = start >= SWAP
                for b in bits:
                    if (first or 0 in XCARRY or swapped) if b == F // 2 else first:
                        give(n, i, start, size, kind(b, 0), at(k, f ^ b, t))
                give(n, i, start, size, 0, at(1 - k, f, t))
            meet()
        greet()
        if cross:
            pl.semaphore_wait(meet_sem.at[top], 1)
        if not last:
            for dev in plane(k + 1):
                send(lnp, lng.at[me], sent.at[0], gain_sem.at[1], dev)
        for _, op in sorted(ops, key=lambda op: op[0]):
            op()
        drain(counts[0], sent.at[0])
        total = sg.shape[1]
        await_bytes(gains.at[pl.ds(0, G - 1)], sent.at[0])
        if last:
            await_bytes(sfin.at[:, pl.ds(0, G - 1)], sent.at[0])
            if P_ > 1:
                drain(total - own_rows, sent.at[0])
        else:
            await_bytes(sin.at[:, pl.ds(0, G)], sent.at[0])
            await_bytes(lng.at[pl.ds(0, G)], sent.at[0])
            drain(total * (T - len(zrelay)), sent.at[0])
            if cross and F > 1:
                drain(2 * sum(c[1] for c in chunks if c[0] >= SWAP), sent.at[0])
            if not first:
                drain(total * T, sent.at[0])

    if not cross:
        for q in range(feeds):
            feed(q, range(1, T), mine)
            if P_ > 1:
                pl.when(k != q)(functools.partial(feed, q, [0], mine))
    if P_ == 1:
        run(True, True)
    else:
        pl.when(k == 0)(lambda: run(True, False))
        pl.when(k == P_ - 1)(lambda: run(False, True))
        if P_ > 2:
            pl.when((k > 0) & (k < P_ - 1))(lambda: run(False, False))

    drain(own_rows * (T - 1 if cross else feeds * T - 1), sent.at[0])
    if P_ > 2:
        pl.when(k >= feeds)(lambda: await_bytes(x_ref, sent.at[0]))
    if P_ > 1:
        pl.when(k < P_ - 1)(lambda: await_bytes(out_ref, out_sem.at[0]))


def plan(sizes, own_rows):
    if sizes[0] == 2 and sizes[2] & (sizes[2] - 1) == 0 and all(sum(split) == own_rows for split in SPLITS):
        rows = [size for split in SPLITS for size in split]
        return [(sum(rows[:i]), size) for i, size in enumerate(rows)], True
    size = min(64, own_rows)
    return [(i * size, size) for i in range(own_rows * sizes[0] // size)], False


def when(chunks, own_rows, cross, kk, n, op):
    if cross and TIMES:
        if op == "prep":
            return TIMES[kk]["C00" if kk else "step"][0] - 0.01
        return TIMES[kk][op][n]
    start, size = chunks[n]
    late = start + size
    mine = late - start // own_rows * own_rows if cross else late
    own = not cross or start // own_rows == kk
    base = 6.6 + 1.4 * late / 64
    s0 = 3 + 0.7 * mine / 64 if own else 5.5 + 0.7 * mine / 64
    s1 = 5.5 + 1.4 * mine / 64 if own else 11.5 + 0.8 * mine / 64
    first = {"S0": s0, "S1": s1, "S2": s1 + 1, "step": s1 + 1.1, "prep": s1 + 1.05, "swap": s1 + 4, "fin": s1 + 6}
    later = {
        "S0": s0, "S1": s1, "C00": base + 3, "ent": base + 6, "ent2": base + 8, "C1": base + 9, "C2": base + 10,
        "prep": base + 2.9, "step": base + 10.1, "swap": base + 13, "fin": base + 15,
    }
    return (later if kk else first)[op]


def local(sizes, inputs, norm_gain, w_value, w_gate, w_taps, ln_gain, ln_shift):
    P_, F, T = sizes
    G = F * T
    own_rows, C = inputs.shape
    TOK = own_rows * P_
    chunks, _ = plan(sizes, own_rows)
    NC = len(chunks)
    D = w_value.shape[1]
    W = w_taps.shape[1]
    head = -(-(W - 1) // 8) * 8
    operands = (inputs, norm_gain, w_value, w_gate, w_taps, ln_gain, ln_shift)
    dma = pltpu.SemaphoreType.DMA
    f32, bf16 = jnp.float32, jnp.bfloat16
    V = pltpu.VMEM
    return pl.pallas_call(
        functools.partial(kernel, sizes),
        out_shape=pltpu.VMEM((own_rows, C), bf16),
        in_specs=[pl.BlockSpec(memory_space=pl.ANY)] * 7,
        out_specs=pl.BlockSpec(memory_space=pltpu.VMEM),
        scratch_shapes=[
            V(inputs.shape, bf16), V(norm_gain.shape, bf16), V((D, 2 * C), bf16), V(w_taps.shape, bf16),
            V(ln_gain.shape, f32), V(ln_shift.shape, f32),
            dma((len(operands),)),
            V((G, TOK, C), bf16), V((G, TOK, C), bf16), V((G, TOK, C), bf16),
            V((G, 1, C), f32), V((G, 2, 1, C), f32),
            V((NC, G, 2, LEN), f32), V((NC, G, 2, LEN), f32), V((NC, 2, LEN), f32),
            V((LEN + head, C), f32), V((W, C), f32),
            V((TOK, C), f32), V((TOK, C), bf16), V((NC, 2, LEN, C), f32), V((2, 1, C), f32), V((TOK, C), bf16),
            V((LEN, LEN), f32),
            dma((NC, T * F)) if F & (F - 1) else dma((NC, max(F // 2, 1) * T + 1)),
            dma((NC, T + 1)), dma((NC, max(F // 2 - 1, 0) * T + 1)), dma((NC,)), dma((NC,)), dma((2,)), dma((1,)),
            dma((1,)), V((TOK, C), bf16), dma((NC,)), pltpu.SemaphoreType.REGULAR((4,)),
        ],
        compiler_params=pltpu.CompilerParams(collective_id=0, has_side_effects=True),
    )(*operands)


def solution(mesh):
    sizes = (mesh.shape["pp"], mesh.shape["fs"], mesh.shape["tp"])
    in_specs = (
        P("pp", ("fs", "tp")),
        P("pp", ("fs", "tp")),
        P("pp", None, ("fs", "tp")),
        P("pp", None, ("fs", "tp")),
        P("pp", None, ("fs", "tp")),
        P("pp", ("fs", "tp")),
        P("pp", ("fs", "tp")),
    )
    out_specs = P("pp", ("fs", "tp"))
    return jax.shard_map(
        functools.partial(local, sizes), mesh=mesh, in_specs=in_specs, out_specs=out_specs,
        check_vma=False,
    )
```

```python
import functools

import jax
import jax.numpy as jnp
from jax import lax
from jax.experimental import pallas as pl
from jax.experimental.pallas import tpu as pltpu
from jax.sharding import PartitionSpec as P

LEN = 128
SPLITS = ((128, 128), (128, 128))
FEED = (1, 2, 3)
SEND = (3, 0, 2, 1)
ENTER = (0, 3, 1, 2)
XCARRY = (1, 2, 3)
ZRELAY = (1, 2)
SWAP = 256
TIMES = (
    {"S0": (-0.48, 4.35, 10.17, 11.39), "S1": (6.67, 11.13, 17.25, 20.33), "S2": (8.5, 15.39, 18.61, 20.55), "step": (8.5, 15.39, 18.61, 20.55), "swap": (0, 0, 26.5, 26.88)},
    {"S0": (10.67, 16.26, 7.57, 7.57), "C00": (16.08, 17.31, 18.47, 19.95), "ent": (18.0, 19.3, 21.72, 24.23), "C1": (21.04, 25.35, 26.83, 31.69), "C2": (21.81, 26.26, 31.37, 33.41), "step": (21.81, 26.27, 31.37, 33.42), "fin": (32.83, 33.0, 38.98, 44.31), "S1": (0, 0, 8.63, 11.78), "ent2": (0, 0, 29.86, 28.1)},
)


norm_eps = 1e-06
layer_eps = 1e-05
MESH = pl.DeviceIdType.MESH


def kernel(
    sizes,
    x_hbm,
    gain_hbm,
    wv_hbm,
    wg_hbm,
    taps_hbm,
    lgain_hbm,
    lshift_hbm,
    out_ref,
    x_ref,
    gain_ref,
    wcat,
    taps_ref,
    lgain_ref,
    lshift_ref,
    load_sem,
    sg,
    cg,
    hg,
    gains,
    lng,
    sin,
    sfin,
    sout,
    pad,
    taps,
    conv_own,
    conv_out,
    keep,
    lnp,
    new_buf,
    turn,
    s_sem,
    c_sem,
    h_sem,
    sin_sem,
    sfin_sem,
    gain_sem,
    out_sem,
    sent,
    side,
    side_sem,
    meet_sem,
):
    P_, F, T = sizes
    G = F * T
    k, f, t = lax.axis_index("pp"), lax.axis_index("fs"), lax.axis_index("tp")
    C = conv_own.shape[1]
    D = wcat.shape[0]
    W = taps.shape[0]
    own_rows = x_ref.shape[0]
    head = pad.shape[0] - LEN
    me = f * T + t
    feeds = min(2, P_)

    loads = [
        pltpu.make_async_copy(a, b, load_sem.at[n])
        for n, (a, b) in enumerate(
            [
                (x_hbm, x_ref), (gain_hbm, gain_ref), (lgain_hbm, lgain_ref), (lshift_hbm, lshift_ref),
                (taps_hbm, taps_ref),
                (wv_hbm.at[0], wcat.at[:, pl.ds(0, C)]), (wg_hbm.at[0], wcat.at[:, pl.ds(C, C)]),
            ]
        )
    ]
    for load in loads:
        load.start()

    if T & (T - 1) == 0:
        to_t = [t] + [t ^ d for d in range(1, T)]
        from_t = to_t
    else:
        to_t = [lax.rem(t + d, T) for d in range(T)]
        from_t = [lax.rem(t + T - d, T) for d in range(T)]

    def at(kk, ff, tt):
        return {"pp": kk, "fs": ff, "tp": tt}

    def send(src, dst, s_sem_, r_sem, dev):
        pltpu.make_async_remote_copy(
            src_ref=src, dst_ref=dst, send_sem=s_sem_, recv_sem=r_sem, device_id=dev, device_id_type=MESH
        ).start()

    def await_bytes(ref, sem):
        pltpu.make_async_copy(ref, ref, sem).wait()

    peers = [at(k, lax.rem(f + df, F), to_t[dt]) for dt in range(T - 1, -1, -1) for df in range(F) if df or dt]

    def plane(kk):
        return [at(kk, lax.rem(f + df, F), to_t[dt]) for dt in range(T - 1, -1, -1) for df in range(F)]

    bits = []
    b = F // 2
    while b:
        bits.append(b)
        b //= 2
    pow2 = T & (T - 1) == 0
    every = tuple(range(T))
    chunks, cross = plan(sizes, own_rows)
    NCH = len(chunks)
    zrelay = ZRELAY if pow2 and T == 4 else ()

    def rows_of(n):
        return pl.ds(chunks[n][0], chunks[n][1])

    def feed(q, dts, mine):
        for n, start, i in mine:
            size = chunks[n][1] if cross else chunks[0][1]
            for dt in dts:
                send(
                    x_ref.at[pl.ds(i, size)], sg.at[me, pl.ds(start, size)], sent.at[0], s_sem.at[n, dt],
                    at(q, f, to_t[dt]),
                )

    def own_copies(mine):
        for n, start, i in mine:
            size = chunks[n][1] if cross else chunks[0][1]
            pltpu.make_async_copy(
                x_hbm.at[pl.ds(i, size)], sg.at[me, pl.ds(start, size)], s_sem.at[n, 0]
            ).start()

    def mine_of(kk):
        return [(n, c, c % own_rows) for n, (c, _) in enumerate(chunks) if c // own_rows == kk]

    if cross:
        for kk in range(P_):
            pl.when(k == kk)(functools.partial(own_copies, mine_of(kk)))
    else:
        size = chunks[0][1]
        mine = [(k * (own_rows // size) + i, k * own_rows + i * size, i * size) for i in range(own_rows // size)]
        if P_ > feeds:
            pl.when(k < feeds)(functools.partial(own_copies, mine))
        else:
            own_copies(mine)
    barrier = pltpu.get_barrier_semaphore()
    column = [at(k, f, tt) for tt in to_t[1:]]
    if cross:
        everyone = column + [at(k, f ^ b, t) for b in bits] + [at(1 - k, f, t)]
    else:
        everyone = peers + [dev for dk in range(1, P_) for dev in plane(lax.rem(k + dk, P_))]
    for dev in everyone:
        pl.semaphore_signal(barrier, inc=1, device_id=dev, device_id_type=MESH)
    for load in loads[:4]:
        load.wait()
    gains[me] = gain_ref[...].astype(jnp.float32)
    lnp[0] = lgain_ref[...] * 0.5
    lnp[1] = lshift_ref[...] * 0.5
    pad[0:head, :] = jnp.zeros((head, C), jnp.float32)
    turn[...] = jnp.zeros_like(turn)
    pl.semaphore_wait(barrier, len(everyone))

    def meet():
        for i, b in enumerate(bits):
            pl.semaphore_signal(meet_sem.at[i], inc=1, device_id=at(k, f ^ b, t), device_id_type=MESH)
            pl.semaphore_wait(meet_sem.at[i], 1)
        pl.semaphore_signal(meet_sem.at[top], inc=1, device_id=at(1 - k, f, t), device_id_type=MESH)

    def give(n, i, start, size, cls, dev):
        send(x_ref.at[pl.ds(i, size)], sg.at[me, pl.ds(start, size)], sent.at[0], s_sem.at[n, cls], dev)
        counts[0] += size

    def introduce(last):
        if cross:
            pl.semaphore_wait(meet_sem.at[top], 1)
        if not last:
            for dev in plane(k + 1):
                send(lnp, lng.at[me], sent.at[0], gain_sem.at[1], dev)

    def greet():
        for dev in peers:
            send(gains.at[me], gains.at[me], sent.at[0], gain_sem.at[0], dev)

    top = len(bits)
    counts = [0]

    def stage(r):
        return 0 if r == 0 else len(bits) - ((r & -r).bit_length() - 1)

    relayed = [r for r in range(F) if not top or stage(r) < top]
    ends = [r for r in range(F) if r not in relayed]

    def kind(r, dt):
        if top and stage(r) == top:
            return len(relayed) * T
        return relayed.index(r) * T + dt

    def forward(buf, sem, n, slot, cls, dev):
        block = buf.at[slot, rows_of(n)]
        send(block, block, sent.at[0], sem.at[n, cls], dev)
        counts[0] += chunks[n][1]

    def arrived(buf, sem, n, slot, cls):
        await_bytes(buf.at[slot, rows_of(n)], sem.at[n, cls])

    def hop(buf, sem, n, lv, dts, ups=every, down=True, over=(), given=False, base=0):
        if top and lv == top:
            await_bytes(buf.at[pl.ds(0, len(ends) * T), rows_of(n)], sem.at[n, kind(ends[0], 0) - base])
            return
        for r in range(F):
            if stage(r) != lv:
                continue
            for dt in dts:
                slot = (f ^ r) * T + from_t[dt]
                arrived(buf, sem, n, slot, kind(r, dt) - base)
                if given and dt == 0:
                    continue
                for b in bits:
                    if b < ((r & -r) or F) and (dt in ups if b == F // 2 else down):
                        forward(buf, sem, n, slot, kind(r ^ b, dt) - base, at(k, f ^ b, t))
                if dt in over:
                    forward(buf, sem, n, slot, kind(r, dt) - base, at(1 - k, f, t))

    def prepare(first):
        if not first:
            await_bytes(lng.at[pl.ds(0, G)], gain_sem.at[1])
        for load in loads[4:]:
            load.wait()
        taps[...] = taps_ref[0].astype(jnp.float32)
        await_bytes(gains.at[pl.ds(0, G - 1)], gain_sem.at[0])
        for s in range(G):
            turn[s : s + 1, :] = gains[s]
        cols = turn[...].T
        for s in range(G):
            rows = pl.ds(s * C, C)
            wcat[rows, :] = (wcat[rows, :].astype(jnp.float32) * cols[:, s : s + 1]).astype(jnp.bfloat16)

    def moments(ref, n):
        R = chunks[n][1]
        turn[0:2, :] = jnp.sum(ref[n], axis=0)
        cols = turn[...].T
        mu = cols[0:R, 0:1] / D
        var = cols[0:R, 1:2] / D - mu * mu
        return mu, lax.rsqrt(var + layer_eps)

    def layer_end(n, slot, mu, rs):
        half = (cg[slot, rows_of(n)].astype(jnp.float32) - mu) * rs * lng[slot, 0] + lng[slot, 1]
        hg[slot, rows_of(n)] = (
            sg[slot, rows_of(n)].astype(jnp.float32) + (half + half * jnp.tanh(half))
        ).astype(jnp.bfloat16)

    def enter(n, swapped):
        await_bytes(sin.at[n, pl.ds(0, G)], sin_sem.at[n])
        mu, rs = moments(sin, n)
        if swapped:
            keep[n, 0, 0 : chunks[n][1], :] = jnp.broadcast_to(mu, (chunks[n][1], C))
            keep[n, 1, 0 : chunks[n][1], :] = jnp.broadcast_to(rs, (chunks[n][1], C))
        for dt in (ENTER if len(ENTER) == T else every):
            slot = f * T + from_t[dt]
            if dt or not zrelay:
                arrived(cg, c_sem, n, slot, dt)
            layer_end(n, slot, mu, rs)
            for b in bits:
                if not (swapped and dt == 0 and b == F // 2):
                    forward(hg, h_sem, n, slot, kind(b, dt) - T, at(k, f ^ b, t))

    def enter_swapped(n):
        slot = (f ^ (F // 2)) * T + t
        arrived(cg, c_sem, n, slot, T)
        layer_end(n, slot, keep[n, 0, 0 : chunks[n][1], :], keep[n, 1, 0 : chunks[n][1], :])
        for b in bits[1:]:
            forward(hg, h_sem, n, slot, kind(F // 2 ^ b, 0) - T, at(k, f ^ b, t))

    def spread(n):
        slot = f * T + t
        arrived(cg, c_sem, n, slot, 0)
        for dz in zrelay:
            forward(cg, c_sem, n, slot, dz, at(k, f, to_t[dz]))

    def project(n, buf):
        start, R = chunks[n]
        blocks = [buf[s, rows_of(n)] for s in range(G)]
        squares = jnp.zeros((R, C), jnp.float32)
        for xb in blocks:
            xf = xb.astype(jnp.float32)
            squares = squares + xf * xf
        scale = lax.rsqrt(jnp.sum(squares, axis=1, keepdims=True) / D + norm_eps)
        both = jnp.dot(jnp.concatenate(blocks, axis=1), wcat[...], preferred_element_type=jnp.float32) * scale
        j = start % LEN
        pad[head + j : head + j + R, :] = both[:, :C] * (0.5 + 0.5 * jnp.tanh(0.5 * both[:, C:]))
        step = 32 if R % 32 == 0 else R
        for r0 in range(0, R, step):
            acc = jnp.zeros((step, C), jnp.float32)
            for w in range(W):
                o = head - (W - 1) + w + j + r0
                acc = acc + pad[o : o + step, :] * taps[w : w + 1, :]
            conv_own[start + r0 : start + r0 + step, :] = acc
        conv = conv_own[start : start + R, :]
        lane = lax.broadcasted_iota(jnp.int32, (R, LEN), 1)
        s1 = jnp.sum(conv, axis=1, keepdims=True)
        s2 = jnp.sum(conv * conv, axis=1, keepdims=True)
        turn[0:R, :] = jnp.where(lane == 0, s1, jnp.where(lane == 1, s2, 0.0))
        return conv, turn[...].T[0:2, :]

    def pass_on(n, first, swapped):
        conv, stat = project(n, sg if first else hg)
        rows = rows_of(n)
        sout[n] = stat
        conv_out[rows, :] = conv.astype(jnp.bfloat16)
        for dev in plane(k + 1):
            send(sout.at[n], sin.at[n, me], sent.at[0], sin_sem.at[n], dev)
        for dt in SEND if len(SEND) == T else every:
            if dt not in zrelay:
                send(conv_out.at[rows], cg.at[me, rows], sent.at[0], c_sem.at[n, dt], at(k + 1, f, to_t[dt]))
        if swapped:
            send(conv_out.at[rows], side.at[rows], sent.at[0], side_sem.at[n], at(k, f ^ (F // 2), t))
        if not first:
            for dt in every:
                send(hg.at[me, rows], sg.at[me, rows], sent.at[0], s_sem.at[n, dt], at(k + 1, f, to_t[dt]))

    def swap_on(n):
        rows = rows_of(n)
        await_bytes(side.at[rows], side_sem.at[n])
        slot = (f ^ (F // 2)) * T + t
        send(side.at[rows], cg.at[slot, rows], sent.at[0], c_sem.at[n, T], at(k + 1, f, t))

    def last_stats(n, first):
        _, stat = project(n, sg if first else hg)
        sfin[n, me] = stat
        for dev in peers:
            send(sfin.at[n, me], sfin.at[n, me], sent.at[0], sfin_sem.at[n], dev)

    def finish(n, first):
        start, R = chunks[n]
        await_bytes(sfin.at[n, pl.ds(0, G - 1)], sfin_sem.at[n])
        mu, rs = moments(sfin, n)
        half = (conv_own[start : start + R, :] - mu) * rs * lnp[0] + lnp[1]
        stream = (sg if first else hg)[me, rows_of(n)]
        new = (stream.astype(jnp.float32) + (half + half * jnp.tanh(half))).astype(jnp.bfloat16)
        owner, i = start // own_rows, start % own_rows
        rows = pl.ds(i, R)
        if owner == P_ - 1:
            out_ref[rows, :] = new
        else:
            new_buf[rows_of(n), :] = new
            send(new_buf.at[rows_of(n)], out_ref.at[rows], sent.at[0], out_sem.at[0], at(owner, f, t))

    def drain(rows, sem):
        full = sg.shape[1]
        while rows >= full:
            m = min(G, rows // full)
            await_bytes(sg.at[pl.ds(0, m)], sem)
            rows -= m * full
        if rows:
            await_bytes(sg.at[0, pl.ds(0, rows)], sem)

    def run(first, last):
        counts[0] = 0
        kk = 0 if first else 1
        ops = []
        for n, (start, size) in enumerate(chunks):
            own = not cross or start // own_rows == kk
            swapped = cross and F > 1 and start >= SWAP
            at_ = functools.partial(when, chunks, own_rows, cross, kk, n)
            x1 = XCARRY if cross else ()
            zero = (0,) if swapped else ()
            if first:
                if own:
                    ops.append((at_("S0"), functools.partial(hop, sg, s_sem, n, 0, every, over=every if cross else (), given=cross)))
                else:
                    ups = tuple(d for d in every if d not in x1)
                    ops.append((at_("S0"), functools.partial(hop, sg, s_sem, n, 0, every, ups)))
                for lv in range(1, top + 1):
                    over = zero if own and lv == 1 else ()
                    ops.append((at_("S%d" % min(lv, 2)), functools.partial(hop, sg, s_sem, n, lv, every, over=over)))
            else:
                if cross and own:
                    ups = tuple(sorted(set(x1 + zero)))
                    ops.append((at_("S0"), functools.partial(hop, sg, s_sem, n, 0, every, ups, False, every, True)))
                    if ups:
                        ops.append((at_("S1"), functools.partial(hop, sg, s_sem, n, 1, ups, (), False, x1)))
                else:
                    ops.append((at_("S0"), functools.partial(hop, sg, s_sem, n, 0, every, (), False)))
                    if swapped:
                        ops.append((at_("S1"), functools.partial(hop, sg, s_sem, n, 1, (0,), (), False)))
                if zrelay:
                    ops.append((at_("C00"), functools.partial(spread, n)))
                ops.append((at_("ent"), functools.partial(enter, n, swapped)))
                if swapped:
                    ops.append((at_("ent2"), functools.partial(enter_swapped, n)))
                for lv in range(1, top + 1):
                    dts = every[1:] if swapped and lv == 1 else every
                    ops.append((at_("C%d" % min(lv, 2)), functools.partial(hop, hg, h_sem, n, lv, dts, base=T)))
            if n == 0:
                ops.append((at_("prep"), functools.partial(prepare, first)))
            if last:
                ops.append((at_("step"), functools.partial(last_stats, n, first)))
                ops.append((at_("fin"), functools.partial(finish, n, first)))
            else:
                ops.append((at_("step"), functools.partial(pass_on, n, first, swapped)))
                if swapped:
                    ops.append((at_("swap"), functools.partial(swap_on, n)))
        if cross:
            for entry in mine_of(kk):
                feed(kk, FEED, [entry])
                n, start, i = entry
                size = chunks[n][1]
                swapped = start >= SWAP
                for b in bits:
                    if (first or 0 in XCARRY or swapped) if b == F // 2 else first:
                        give(n, i, start, size, kind(b, 0), at(k, f ^ b, t))
                give(n, i, start, size, 0, at(1 - k, f, t))
            meet()
        greet()
        soon = min(op[0] for op in ops)
        ops.append((soon + 1e-6, functools.partial(introduce, last)))
        for _, op in sorted(ops, key=lambda op: op[0]):
            op()
        drain(counts[0], sent.at[0])
        total = sg.shape[1]
        await_bytes(gains.at[pl.ds(0, G - 1)], sent.at[0])
        if last:
            await_bytes(sfin.at[:, pl.ds(0, G - 1)], sent.at[0])
            if P_ > 1:
                drain(total - own_rows, sent.at[0])
        else:
            await_bytes(sin.at[:, pl.ds(0, G)], sent.at[0])
            await_bytes(lng.at[pl.ds(0, G)], sent.at[0])
            drain(total * (T - len(zrelay)), sent.at[0])
            if cross and F > 1:
                drain(2 * sum(c[1] for c in chunks if c[0] >= SWAP), sent.at[0])
            if not first:
                drain(total * T, sent.at[0])

    if not cross:
        for q in range(feeds):
            feed(q, range(1, T), mine)
            if P_ > 1:
                pl.when(k != q)(functools.partial(feed, q, [0], mine))
    if P_ == 1:
        run(True, True)
    else:
        pl.when(k == 0)(lambda: run(True, False))
        pl.when(k == P_ - 1)(lambda: run(False, True))
        if P_ > 2:
            pl.when((k > 0) & (k < P_ - 1))(lambda: run(False, False))

    drain(own_rows * (T - 1 if cross else feeds * T - 1), sent.at[0])
    if P_ > 2:
        pl.when(k >= feeds)(lambda: await_bytes(x_ref, sent.at[0]))
    if P_ > 1:
        pl.when(k < P_ - 1)(lambda: await_bytes(out_ref, out_sem.at[0]))


def plan(sizes, own_rows):
    if sizes[0] == 2 and sizes[2] & (sizes[2] - 1) == 0 and all(sum(split) == own_rows for split in SPLITS):
        rows = [size for split in SPLITS for size in split]
        return [(sum(rows[:i]), size) for i, size in enumerate(rows)], True
    size = min(64, own_rows)
    return [(i * size, size) for i in range(own_rows * sizes[0] // size)], False


def when(chunks, own_rows, cross, kk, n, op):
    if cross and TIMES:
        if op == "prep":
            return TIMES[kk]["C00" if kk else "step"][0] - 0.01
        return TIMES[kk][op][n]
    start, size = chunks[n]
    late = start + size
    mine = late - start // own_rows * own_rows if cross else late
    own = not cross or start // own_rows == kk
    base = 6.6 + 1.4 * late / 64
    s0 = 3 + 0.7 * mine / 64 if own else 5.5 + 0.7 * mine / 64
    s1 = 5.5 + 1.4 * mine / 64 if own else 11.5 + 0.8 * mine / 64
    first = {"S0": s0, "S1": s1, "S2": s1 + 1, "step": s1 + 1.1, "prep": s1 + 1.05, "swap": s1 + 4, "fin": s1 + 6}
    later = {
        "S0": s0, "S1": s1, "C00": base + 3, "ent": base + 6, "ent2": base + 8, "C1": base + 9, "C2": base + 10,
        "prep": base + 2.9, "step": base + 10.1, "swap": base + 13, "fin": base + 15,
    }
    return (later if kk else first)[op]


def local(sizes, inputs, norm_gain, w_value, w_gate, w_taps, ln_gain, ln_shift):
    P_, F, T = sizes
    G = F * T
    own_rows, C = inputs.shape
    TOK = own_rows * P_
    chunks, _ = plan(sizes, own_rows)
    NC = len(chunks)
    D = w_value.shape[1]
    W = w_taps.shape[1]
    head = -(-(W - 1) // 8) * 8
    operands = (inputs, norm_gain, w_value, w_gate, w_taps, ln_gain, ln_shift)
    dma = pltpu.SemaphoreType.DMA
    f32, bf16 = jnp.float32, jnp.bfloat16
    V = pltpu.VMEM
    return pl.pallas_call(
        functools.partial(kernel, sizes),
        out_shape=pltpu.VMEM((own_rows, C), bf16),
        in_specs=[pl.BlockSpec(memory_space=pl.ANY)] * 7,
        out_specs=pl.BlockSpec(memory_space=pltpu.VMEM),
        scratch_shapes=[
            V(inputs.shape, bf16), V(norm_gain.shape, bf16), V((D, 2 * C), bf16), V(w_taps.shape, bf16),
            V(ln_gain.shape, f32), V(ln_shift.shape, f32),
            dma((len(operands),)),
            V((G, TOK, C), bf16), V((G, TOK, C), bf16), V((G, TOK, C), bf16),
            V((G, 1, C), f32), V((G, 2, 1, C), f32),
            V((NC, G, 2, LEN), f32), V((NC, G, 2, LEN), f32), V((NC, 2, LEN), f32),
            V((LEN + head, C), f32), V((W, C), f32),
            V((TOK, C), f32), V((TOK, C), bf16), V((NC, 2, LEN, C), f32), V((2, 1, C), f32), V((TOK, C), bf16),
            V((LEN, LEN), f32),
            dma((NC, T * F)) if F & (F - 1) else dma((NC, max(F // 2, 1) * T + 1)),
            dma((NC, T + 1)), dma((NC, max(F // 2 - 1, 0) * T + 1)), dma((NC,)), dma((NC,)), dma((2,)), dma((1,)),
            dma((1,)), V((TOK, C), bf16), dma((NC,)), pltpu.SemaphoreType.REGULAR((4,)),
        ],
        compiler_params=pltpu.CompilerParams(collective_id=0, has_side_effects=True),
    )(*operands)


def solution(mesh):
    sizes = (mesh.shape["pp"], mesh.shape["fs"], mesh.shape["tp"])
    in_specs = (
        P("pp", ("fs", "tp")),
        P("pp", ("fs", "tp")),
        P("pp", None, ("fs", "tp")),
        P("pp", None, ("fs", "tp")),
        P("pp", None, ("fs", "tp")),
        P("pp", ("fs", "tp")),
        P("pp", ("fs", "tp")),
    )
    out_specs = P("pp", ("fs", "tp"))
    return jax.shard_map(
        functools.partial(local, sizes), mesh=mesh, in_specs=in_specs, out_specs=out_specs,
        check_vma=False,
    )
```

```python
import functools

import jax
import jax.numpy as jnp
from jax import lax
from jax.experimental import pallas as pl
from jax.experimental.pallas import tpu as pltpu
from jax.sharding import PartitionSpec as P

LEN = 128
SPLITS = ((128, 128), (128, 128))
FEED = (1, 2, 3)
SEND = (3, 0, 2, 1)
ENTER = (0, 3, 1, 2)
XCARRY = (1, 2, 3)
ZRELAY = (1, 2)
SWAP = 256
TIMES = (
    {"S0": (-0.48, 4.35, 10.17, 11.39), "S1": (6.67, 11.13, 17.25, 20.33), "S2": (8.5, 15.39, 18.61, 20.55), "step": (8.5, 15.39, 18.61, 20.55), "swap": (0, 0, 26.5, 26.88)},
    {"S0": (10.67, 16.26, 7.57, 7.57), "C00": (16.08, 17.31, 18.47, 19.95), "ent": (18.0, 19.3, 21.72, 24.23), "C1": (21.04, 25.35, 26.83, 31.69), "C2": (21.81, 26.26, 31.37, 33.41), "step": (21.81, 26.27, 31.37, 33.42), "fin": (32.83, 33.0, 38.98, 44.31), "S1": (0, 0, 8.63, 11.78), "ent2": (0, 0, 29.86, 28.1)},
)


norm_eps = 1e-06
layer_eps = 1e-05
MESH = pl.DeviceIdType.MESH


def kernel(
    sizes,
    x_hbm,
    gain_hbm,
    wv_hbm,
    wg_hbm,
    taps_hbm,
    lgain_hbm,
    lshift_hbm,
    out_ref,
    x_ref,
    gain_ref,
    wcat,
    taps_ref,
    lgain_ref,
    lshift_ref,
    load_sem,
    sg,
    cg,
    hg,
    gains,
    lng,
    sin,
    sfin,
    sout,
    pad,
    taps,
    conv_own,
    conv_out,
    keep,
    lnp,
    new_buf,
    turn,
    s_sem,
    c_sem,
    h_sem,
    sin_sem,
    sfin_sem,
    gain_sem,
    out_sem,
    sent,
    side,
    side_sem,
    meet_sem,
):
    P_, F, T = sizes
    G = F * T
    k, f, t = lax.axis_index("pp"), lax.axis_index("fs"), lax.axis_index("tp")
    C = conv_own.shape[1]
    D = wcat.shape[0]
    W = taps.shape[0]
    own_rows = x_ref.shape[0]
    head = pad.shape[0] - LEN
    me = f * T + t
    feeds = min(2, P_)

    loads = [
        pltpu.make_async_copy(a, b, load_sem.at[n])
        for n, (a, b) in enumerate(
            [
                (x_hbm, x_ref), (gain_hbm, gain_ref), (lgain_hbm, lgain_ref), (lshift_hbm, lshift_ref),
                (taps_hbm, taps_ref),
                (wv_hbm.at[0], wcat.at[:, pl.ds(0, C)]), (wg_hbm.at[0], wcat.at[:, pl.ds(C, C)]),
            ]
        )
    ]
    for load in loads:
        load.start()

    if T & (T - 1) == 0:
        to_t = [t] + [t ^ d for d in range(1, T)]
        from_t = to_t
    else:
        to_t = [lax.rem(t + d, T) for d in range(T)]
        from_t = [lax.rem(t + T - d, T) for d in range(T)]

    def at(kk, ff, tt):
        return {"pp": kk, "fs": ff, "tp": tt}

    def send(src, dst, s_sem_, r_sem, dev):
        pltpu.make_async_remote_copy(
            src_ref=src, dst_ref=dst, send_sem=s_sem_, recv_sem=r_sem, device_id=dev, device_id_type=MESH
        ).start()

    def await_bytes(ref, sem):
        pltpu.make_async_copy(ref, ref, sem).wait()

    peers = [at(k, lax.rem(f + df, F), to_t[dt]) for dt in range(T - 1, -1, -1) for df in range(F) if df or dt]

    def plane(kk):
        return [at(kk, lax.rem(f + df, F), to_t[dt]) for dt in range(T - 1, -1, -1) for df in range(F)]

    bits = []
    b = F // 2
    while b:
        bits.append(b)
        b //= 2
    pow2 = T & (T - 1) == 0
    every = tuple(range(T))
    chunks, cross = plan(sizes, own_rows)
    NCH = len(chunks)
    zrelay = ZRELAY if pow2 and T == 4 else ()

    def rows_of(n):
        return pl.ds(chunks[n][0], chunks[n][1])

    def feed(q, dts, mine):
        for n, start, i in mine:
            size = chunks[n][1] if cross else chunks[0][1]
            for dt in dts:
                send(
                    x_ref.at[pl.ds(i, size)], sg.at[me, pl.ds(start, size)], sent.at[0], s_sem.at[n, dt],
                    at(q, f, to_t[dt]),
                )

    def own_copies(mine):
        for n, start, i in mine:
            size = chunks[n][1] if cross else chunks[0][1]
            pltpu.make_async_copy(
                x_hbm.at[pl.ds(i, size)], sg.at[me, pl.ds(start, size)], s_sem.at[n, 0]
            ).start()

    def mine_of(kk):
        return [(n, c, c % own_rows) for n, (c, _) in enumerate(chunks) if c // own_rows == kk]

    if cross:
        for kk in range(P_):
            pl.when(k == kk)(functools.partial(own_copies, mine_of(kk)))
    else:
        size = chunks[0][1]
        mine = [(k * (own_rows // size) + i, k * own_rows + i * size, i * size) for i in range(own_rows // size)]
        if P_ > feeds:
            pl.when(k < feeds)(functools.partial(own_copies, mine))
        else:
            own_copies(mine)
    barrier = pltpu.get_barrier_semaphore()
    column = [at(k, f, tt) for tt in to_t[1:]]
    if cross:
        everyone = column + [at(k, f ^ b, t) for b in bits] + [at(1 - k, f, t)]
    else:
        everyone = peers + [dev for dk in range(1, P_) for dev in plane(lax.rem(k + dk, P_))]
    for dev in everyone:
        pl.semaphore_signal(barrier, inc=1, device_id=dev, device_id_type=MESH)
    for load in loads[:4]:
        load.wait()
    gains[me] = gain_ref[...].astype(jnp.float32)
    lnp[0] = lgain_ref[...] * 0.5
    lnp[1] = lshift_ref[...] * 0.5
    pad[0:head, :] = jnp.zeros((head, C), jnp.float32)
    turn[...] = jnp.zeros_like(turn)
    pl.semaphore_wait(barrier, len(everyone))

    def meet():
        for i, b in enumerate(bits):
            pl.semaphore_signal(meet_sem.at[i], inc=1, device_id=at(k, f ^ b, t), device_id_type=MESH)
            pl.semaphore_wait(meet_sem.at[i], 1)
        pl.semaphore_signal(meet_sem.at[top], inc=1, device_id=at(1 - k, f, t), device_id_type=MESH)

    def give(n, i, start, size, cls, dev):
        send(x_ref.at[pl.ds(i, size)], sg.at[me, pl.ds(start, size)], sent.at[0], s_sem.at[n, cls], dev)
        counts[0] += size

    def introduce(last):
        if cross:
            pl.semaphore_wait(meet_sem.at[top], 1)
        if not last:
            for dev in plane(k + 1):
                send(lnp, lng.at[me], sent.at[0], gain_sem.at[1], dev)

    def greet():
        for dev in peers:
            send(gains.at[me], gains.at[me], sent.at[0], gain_sem.at[0], dev)

    top = len(bits)
    counts = [0]

    def stage(r):
        return 0 if r == 0 else len(bits) - ((r & -r).bit_length() - 1)

    relayed = [r for r in range(F) if not top or stage(r) < top]
    ends = [r for r in range(F) if r not in relayed]

    def kind(r, dt):
        if top and stage(r) == top:
            return len(relayed) * T
        return relayed.index(r) * T + dt

    def forward(buf, sem, n, slot, cls, dev):
        block = buf.at[slot, rows_of(n)]
        send(block, block, sent.at[0], sem.at[n, cls], dev)
        counts[0] += chunks[n][1]

    def arrived(buf, sem, n, slot, cls):
        await_bytes(buf.at[slot, rows_of(n)], sem.at[n, cls])

    def hop(buf, sem, n, lv, dts, ups=every, down=True, over=(), given=False, base=0):
        if top and lv == top:
            await_bytes(buf.at[pl.ds(0, len(ends) * T), rows_of(n)], sem.at[n, kind(ends[0], 0) - base])
            return
        for r in range(F):
            if stage(r) != lv:
                continue
            for dt in dts:
                slot = (f ^ r) * T + from_t[dt]
                arrived(buf, sem, n, slot, kind(r, dt) - base)
                if given and dt == 0:
                    continue
                for b in bits:
                    if b < ((r & -r) or F) and (dt in ups if b == F // 2 else down):
                        forward(buf, sem, n, slot, kind(r ^ b, dt) - base, at(k, f ^ b, t))
                if dt in over:
                    forward(buf, sem, n, slot, kind(r, dt) - base, at(1 - k, f, t))

    def prepare(first):
        if not first:
            await_bytes(lng.at[pl.ds(0, G)], gain_sem.at[1])
        for load in loads[4:]:
            load.wait()
        taps[...] = taps_ref[0].astype(jnp.float32)
        await_bytes(gains.at[pl.ds(0, G - 1)], gain_sem.at[0])
        for s in range(G):
            turn[s : s + 1, :] = gains[s]
        cols = turn[...].T
        for s in range(G):
            rows = pl.ds(s * C, C)
            wcat[rows, :] = (wcat[rows, :].astype(jnp.float32) * cols[:, s : s + 1]).astype(jnp.bfloat16)

    def moments(ref, n):
        R = chunks[n][1]
        turn[0:2, :] = jnp.sum(ref[n], axis=0)
        cols = turn[...].T
        mu = cols[0:R, 0:1] / D
        var = cols[0:R, 1:2] / D - mu * mu
        return mu, lax.rsqrt(var + layer_eps)

    def layer_end(n, slot, mu, rs):
        half = (cg[slot, rows_of(n)].astype(jnp.float32) - mu) * rs * lng[slot, 0] + lng[slot, 1]
        hg[slot, rows_of(n)] = (
            sg[slot, rows_of(n)].astype(jnp.float32) + (half + half * jnp.tanh(half))
        ).astype(jnp.bfloat16)

    def enter(n, swapped):
        await_bytes(sin.at[n, pl.ds(0, G)], sin_sem.at[n])
        mu, rs = moments(sin, n)
        if swapped:
            keep[n, 0, 0 : chunks[n][1], :] = jnp.broadcast_to(mu, (chunks[n][1], C))
            keep[n, 1, 0 : chunks[n][1], :] = jnp.broadcast_to(rs, (chunks[n][1], C))
        for dt in (ENTER if len(ENTER) == T else every):
            slot = f * T + from_t[dt]
            if dt or not zrelay:
                arrived(cg, c_sem, n, slot, dt)
            layer_end(n, slot, mu, rs)
            for b in bits:
                if not (swapped and dt == 0 and b == F // 2):
                    forward(hg, h_sem, n, slot, kind(b, dt) - T, at(k, f ^ b, t))

    def enter_swapped(n):
        slot = (f ^ (F // 2)) * T + t
        arrived(cg, c_sem, n, slot, T)
        layer_end(n, slot, keep[n, 0, 0 : chunks[n][1], :], keep[n, 1, 0 : chunks[n][1], :])
        for b in bits[1:]:
            forward(hg, h_sem, n, slot, kind(F // 2 ^ b, 0) - T, at(k, f ^ b, t))

    def spread(n):
        slot = f * T + t
        arrived(cg, c_sem, n, slot, 0)
        for dz in zrelay:
            forward(cg, c_sem, n, slot, dz, at(k, f, to_t[dz]))

    def project(n, buf):
        start, R = chunks[n]
        blocks = [buf[s, rows_of(n)] for s in range(G)]
        squares = jnp.zeros((R, C), jnp.float32)
        for xb in blocks:
            xf = xb.astype(jnp.float32)
            squares = squares + xf * xf
        scale = lax.rsqrt(jnp.sum(squares, axis=1, keepdims=True) / D + norm_eps)
        both = jnp.dot(jnp.concatenate(blocks, axis=1), wcat[...], preferred_element_type=jnp.float32) * scale
        j = start % LEN
        pad[head + j : head + j + R, :] = both[:, :C] * (0.5 + 0.5 * jnp.tanh(0.5 * both[:, C:]))
        step = 32 if R % 32 == 0 else R
        for r0 in range(0, R, step):
            acc = jnp.zeros((step, C), jnp.float32)
            for w in range(W):
                o = head - (W - 1) + w + j + r0
                acc = acc + pad[o : o + step, :] * taps[w : w + 1, :]
            conv_own[start + r0 : start + r0 + step, :] = acc
        conv = conv_own[start : start + R, :]
        lane = lax.broadcasted_iota(jnp.int32, (R, LEN), 1)
        s1 = jnp.sum(conv, axis=1, keepdims=True)
        s2 = jnp.sum(conv * conv, axis=1, keepdims=True)
        turn[0:R, :] = jnp.where(lane == 0, s1, jnp.where(lane == 1, s2, 0.0))
        return conv, turn[...].T[0:2, :]

    def pass_on(n, first, swapped):
        conv, stat = project(n, sg if first else hg)
        rows = rows_of(n)
        sout[n] = stat
        conv_out[rows, :] = conv.astype(jnp.bfloat16)
        for dev in plane(k + 1):
            send(sout.at[n], sin.at[n, me], sent.at[0], sin_sem.at[n], dev)
        for dt in SEND if len(SEND) == T else every:
            if dt not in zrelay:
                send(conv_out.at[rows], cg.at[me, rows], sent.at[0], c_sem.at[n, dt], at(k + 1, f, to_t[dt]))
        if swapped:
            send(conv_out.at[rows], side.at[rows], sent.at[0], side_sem.at[n], at(k, f ^ (F // 2), t))
        if not first:
            for dt in every:
                send(hg.at[me, rows], sg.at[me, rows], sent.at[0], s_sem.at[n, dt], at(k + 1, f, to_t[dt]))

    def swap_on(n):
        rows = rows_of(n)
        await_bytes(side.at[rows], side_sem.at[n])
        slot = (f ^ (F // 2)) * T + t
        send(side.at[rows], cg.at[slot, rows], sent.at[0], c_sem.at[n, T], at(k + 1, f, t))

    def last_stats(n, first):
        _, stat = project(n, sg if first else hg)
        sfin[n, me] = stat
        for dev in peers:
            send(sfin.at[n, me], sfin.at[n, me], sent.at[0], sfin_sem.at[n], dev)

    def finish(n, first):
        start, R = chunks[n]
        await_bytes(sfin.at[n, pl.ds(0, G - 1)], sfin_sem.at[n])
        mu, rs = moments(sfin, n)
        half = (conv_own[start : start + R, :] - mu) * rs * lnp[0] + lnp[1]
        stream = (sg if first else hg)[me, rows_of(n)]
        new = (stream.astype(jnp.float32) + (half + half * jnp.tanh(half))).astype(jnp.bfloat16)
        owner, i = start // own_rows, start % own_rows
        rows = pl.ds(i, R)
        if owner == P_ - 1:
            out_ref[rows, :] = new
        else:
            new_buf[rows_of(n), :] = new
            send(new_buf.at[rows_of(n)], out_ref.at[rows], sent.at[0], out_sem.at[0], at(owner, f, t))

    def drain(rows, sem):
        full = sg.shape[1]
        while rows >= full:
            m = min(G, rows // full)
            await_bytes(sg.at[pl.ds(0, m)], sem)
            rows -= m * full
        if rows:
            await_bytes(sg.at[0, pl.ds(0, rows)], sem)

    def run(first, last):
        counts[0] = 0
        kk = 0 if first else 1
        ops = []
        for n, (start, size) in enumerate(chunks):
            own = not cross or start // own_rows == kk
            swapped = cross and F > 1 and start >= SWAP
            at_ = functools.partial(when, chunks, own_rows, cross, kk, n)
            x1 = XCARRY if cross else ()
            zero = (0,) if swapped else ()
            if first:
                if own:
                    ops.append((at_("S0"), functools.partial(hop, sg, s_sem, n, 0, every, over=every if cross else (), given=cross)))
                else:
                    ups = tuple(d for d in every if d not in x1)
                    ops.append((at_("S0"), functools.partial(hop, sg, s_sem, n, 0, every, ups)))
                for lv in range(1, top + 1):
                    over = zero if own and lv == 1 else ()
                    ops.append((at_("S%d" % min(lv, 2)), functools.partial(hop, sg, s_sem, n, lv, every, over=over)))
            else:
                if cross and own:
                    ups = tuple(sorted(set(x1 + zero)))
                    ops.append((at_("S0"), functools.partial(hop, sg, s_sem, n, 0, every, ups, False, every, True)))
                    if ups:
                        ops.append((at_("S1"), functools.partial(hop, sg, s_sem, n, 1, ups, (), False, x1)))
                else:
                    ops.append((at_("S0"), functools.partial(hop, sg, s_sem, n, 0, every, (), False)))
                    if swapped:
                        ops.append((at_("S1"), functools.partial(hop, sg, s_sem, n, 1, (0,), (), False)))
                if zrelay:
                    ops.append((at_("C00"), functools.partial(spread, n)))
                ops.append((at_("ent"), functools.partial(enter, n, swapped)))
                if swapped:
                    ops.append((at_("ent2"), functools.partial(enter_swapped, n)))
                for lv in range(1, top + 1):
                    dts = every[1:] if swapped and lv == 1 else every
                    ops.append((at_("C%d" % min(lv, 2)), functools.partial(hop, hg, h_sem, n, lv, dts, base=T)))
            if n == 0:
                ops.append((at_("prep"), functools.partial(prepare, first)))
            if last:
                ops.append((at_("step"), functools.partial(last_stats, n, first)))
                ops.append((at_("fin"), functools.partial(finish, n, first)))
            else:
                ops.append((at_("step"), functools.partial(pass_on, n, first, swapped)))
                if swapped:
                    ops.append((at_("swap"), functools.partial(swap_on, n)))
        if cross:
            for entry in mine_of(kk):
                feed(kk, FEED, [entry])
                n, start, i = entry
                size = chunks[n][1]
                swapped = start >= SWAP
                for b in bits:
                    if (first or 0 in XCARRY or swapped) if b == F // 2 else first:
                        give(n, i, start, size, kind(b, 0), at(k, f ^ b, t))
                give(n, i, start, size, 0, at(1 - k, f, t))
            meet()
        greet()
        soon = min(op[0] for op in ops)
        ops.append((soon + 1e-6, functools.partial(introduce, last)))
        for _, op in sorted(ops, key=lambda op: op[0]):
            op()
        drain(counts[0], sent.at[0])
        total = sg.shape[1]
        await_bytes(gains.at[pl.ds(0, G - 1)], sent.at[0])
        if last:
            await_bytes(sfin.at[:, pl.ds(0, G - 1)], sent.at[0])
            if P_ > 1:
                drain(total - own_rows, sent.at[0])
        else:
            await_bytes(sin.at[:, pl.ds(0, G)], sent.at[0])
            await_bytes(lng.at[pl.ds(0, G)], sent.at[0])
            drain(total * (T - len(zrelay)), sent.at[0])
            if cross and F > 1:
                drain(2 * sum(c[1] for c in chunks if c[0] >= SWAP), sent.at[0])
            if not first:
                drain(total * T, sent.at[0])

    if not cross:
        for q in range(feeds):
            feed(q, range(1, T), mine)
            if P_ > 1:
                pl.when(k != q)(functools.partial(feed, q, [0], mine))
    if P_ == 1:
        run(True, True)
    else:
        pl.when(k == 0)(lambda: run(True, False))
        pl.when(k == P_ - 1)(lambda: run(False, True))
        if P_ > 2:
            pl.when((k > 0) & (k < P_ - 1))(lambda: run(False, False))

    drain(own_rows * (T - 1 if cross else feeds * T - 1), sent.at[0])
    if P_ > 2:
        pl.when(k >= feeds)(lambda: await_bytes(x_ref, sent.at[0]))
    if P_ > 1:
        pl.when(k < P_ - 1)(lambda: await_bytes(out_ref, out_sem.at[0]))


def plan(sizes, own_rows):
    if sizes[0] == 2 and sizes[2] & (sizes[2] - 1) == 0 and all(sum(split) == own_rows for split in SPLITS):
        rows = [size for split in SPLITS for size in split]
        return [(sum(rows[:i]), size) for i, size in enumerate(rows)], True
    size = min(64, own_rows)
    return [(i * size, size) for i in range(own_rows * sizes[0] // size)], False


def when(chunks, own_rows, cross, kk, n, op):
    if cross and TIMES:
        if op == "prep":
            return TIMES[kk]["C00" if kk else "S1"][0] - 0.01
        return TIMES[kk][op][n]
    start, size = chunks[n]
    late = start + size
    mine = late - start // own_rows * own_rows if cross else late
    own = not cross or start // own_rows == kk
    base = 6.6 + 1.4 * late / 64
    s0 = 3 + 0.7 * mine / 64 if own else 5.5 + 0.7 * mine / 64
    s1 = 5.5 + 1.4 * mine / 64 if own else 11.5 + 0.8 * mine / 64
    first = {"S0": s0, "S1": s1, "S2": s1 + 1, "step": s1 + 1.1, "prep": s1 + 1.05, "swap": s1 + 4, "fin": s1 + 6}
    later = {
        "S0": s0, "S1": s1, "C00": base + 3, "ent": base + 6, "ent2": base + 8, "C1": base + 9, "C2": base + 10,
        "prep": base + 2.9, "step": base + 10.1, "swap": base + 13, "fin": base + 15,
    }
    return (later if kk else first)[op]


def local(sizes, inputs, norm_gain, w_value, w_gate, w_taps, ln_gain, ln_shift):
    P_, F, T = sizes
    G = F * T
    own_rows, C = inputs.shape
    TOK = own_rows * P_
    chunks, _ = plan(sizes, own_rows)
    NC = len(chunks)
    D = w_value.shape[1]
    W = w_taps.shape[1]
    head = -(-(W - 1) // 8) * 8
    operands = (inputs, norm_gain, w_value, w_gate, w_taps, ln_gain, ln_shift)
    dma = pltpu.SemaphoreType.DMA
    f32, bf16 = jnp.float32, jnp.bfloat16
    V = pltpu.VMEM
    return pl.pallas_call(
        functools.partial(kernel, sizes),
        out_shape=pltpu.VMEM((own_rows, C), bf16),
        in_specs=[pl.BlockSpec(memory_space=pl.ANY)] * 7,
        out_specs=pl.BlockSpec(memory_space=pltpu.VMEM),
        scratch_shapes=[
            V(inputs.shape, bf16), V(norm_gain.shape, bf16), V((D, 2 * C), bf16), V(w_taps.shape, bf16),
            V(ln_gain.shape, f32), V(ln_shift.shape, f32),
            dma((len(operands),)),
            V((G, TOK, C), bf16), V((G, TOK, C), bf16), V((G, TOK, C), bf16),
            V((G, 1, C), f32), V((G, 2, 1, C), f32),
            V((NC, G, 2, LEN), f32), V((NC, G, 2, LEN), f32), V((NC, 2, LEN), f32),
            V((LEN + head, C), f32), V((W, C), f32),
            V((TOK, C), f32), V((TOK, C), bf16), V((NC, 2, LEN, C), f32), V((2, 1, C), f32), V((TOK, C), bf16),
            V((LEN, LEN), f32),
            dma((NC, T * F)) if F & (F - 1) else dma((NC, max(F // 2, 1) * T + 1)),
            dma((NC, T + 1)), dma((NC, max(F // 2 - 1, 0) * T + 1)), dma((NC,)), dma((NC,)), dma((2,)), dma((1,)),
            dma((1,)), V((TOK, C), bf16), dma((NC,)), pltpu.SemaphoreType.REGULAR((4,)),
        ],
        compiler_params=pltpu.CompilerParams(collective_id=0, has_side_effects=True),
    )(*operands)


def solution(mesh):
    sizes = (mesh.shape["pp"], mesh.shape["fs"], mesh.shape["tp"])
    in_specs = (
        P("pp", ("fs", "tp")),
        P("pp", ("fs", "tp")),
        P("pp", None, ("fs", "tp")),
        P("pp", None, ("fs", "tp")),
        P("pp", None, ("fs", "tp")),
        P("pp", ("fs", "tp")),
        P("pp", ("fs", "tp")),
    )
    out_specs = P("pp", ("fs", "tp"))
    return jax.shard_map(
        functools.partial(local, sizes), mesh=mesh, in_specs=in_specs, out_specs=out_specs,
        check_vma=False,
    )
```

```python
import functools

import jax
import jax.numpy as jnp
from jax import lax
from jax.experimental import pallas as pl
from jax.experimental.pallas import tpu as pltpu
from jax.sharding import PartitionSpec as P

LEN = 128
SPLITS = ((128, 128), (128, 128))
FEED = (1, 2, 3)
SEND = (3, 0, 2, 1)
ENTER = (0, 3, 1, 2)
XCARRY = (1, 2, 3)
ZRELAY = (1, 2)
SWAP = 256
TIMES = (
    {"S0": (-0.48, 4.35, 10.17, 11.39), "S1": (6.67, 11.13, 17.25, 20.33), "S2": (8.5, 15.39, 18.61, 20.55), "step": (8.5, 15.39, 18.61, 20.55), "swap": (0, 0, 26.5, 26.88)},
    {"S0": (10.67, 16.26, 7.57, 7.57), "C00": (16.08, 17.31, 18.47, 19.95), "ent": (18.0, 19.3, 21.72, 24.23), "C1": (21.04, 25.35, 26.83, 31.69), "C2": (21.81, 26.26, 31.37, 33.41), "step": (21.81, 26.27, 31.37, 33.42), "fin": (32.83, 34.11, 38.98, 44.31), "S1": (0, 0, 8.63, 11.78), "ent2": (0, 0, 29.86, 28.1)},
)


norm_eps = 1e-06
layer_eps = 1e-05
MESH = pl.DeviceIdType.MESH


def kernel(
    sizes,
    x_hbm,
    gain_hbm,
    wv_hbm,
    wg_hbm,
    taps_hbm,
    lgain_hbm,
    lshift_hbm,
    out_ref,
    x_ref,
    gain_ref,
    wcat,
    taps_ref,
    lgain_ref,
    lshift_ref,
    load_sem,
    sg,
    cg,
    hg,
    gains,
    lng,
    sin,
    sfin,
    sout,
    pad,
    taps,
    conv_own,
    conv_out,
    keep,
    lnp,
    new_buf,
    turn,
    s_sem,
    c_sem,
    h_sem,
    sin_sem,
    sfin_sem,
    gain_sem,
    out_sem,
    sent,
    side,
    side_sem,
    meet_sem,
):
    P_, F, T = sizes
    G = F * T
    k, f, t = lax.axis_index("pp"), lax.axis_index("fs"), lax.axis_index("tp")
    C = conv_own.shape[1]
    D = wcat.shape[0]
    W = taps.shape[0]
    own_rows = x_ref.shape[0]
    head = pad.shape[0] - LEN
    me = f * T + t
    feeds = min(2, P_)

    loads = [
        pltpu.make_async_copy(a, b, load_sem.at[n])
        for n, (a, b) in enumerate(
            [
                (x_hbm, x_ref), (gain_hbm, gain_ref), (lgain_hbm, lgain_ref), (lshift_hbm, lshift_ref),
                (taps_hbm, taps_ref),
                (wv_hbm.at[0], wcat.at[:, pl.ds(0, C)]), (wg_hbm.at[0], wcat.at[:, pl.ds(C, C)]),
            ]
        )
    ]
    for load in loads:
        load.start()

    if T & (T - 1) == 0:
        to_t = [t] + [t ^ d for d in range(1, T)]
        from_t = to_t
    else:
        to_t = [lax.rem(t + d, T) for d in range(T)]
        from_t = [lax.rem(t + T - d, T) for d in range(T)]

    def at(kk, ff, tt):
        return {"pp": kk, "fs": ff, "tp": tt}

    def send(src, dst, s_sem_, r_sem, dev):
        pltpu.make_async_remote_copy(
            src_ref=src, dst_ref=dst, send_sem=s_sem_, recv_sem=r_sem, device_id=dev, device_id_type=MESH
        ).start()

    def await_bytes(ref, sem):
        pltpu.make_async_copy(ref, ref, sem).wait()

    peers = [at(k, lax.rem(f + df, F), to_t[dt]) for dt in range(T - 1, -1, -1) for df in range(F) if df or dt]

    def plane(kk):
        return [at(kk, lax.rem(f + df, F), to_t[dt]) for dt in range(T - 1, -1, -1) for df in range(F)]

    bits = []
    b = F // 2
    while b:
        bits.append(b)
        b //= 2
    pow2 = T & (T - 1) == 0
    every = tuple(range(T))
    chunks, cross = plan(sizes, own_rows)
    NCH = len(chunks)
    zrelay = ZRELAY if pow2 and T == 4 else ()

    def rows_of(n):
        return pl.ds(chunks[n][0], chunks[n][1])

    def feed(q, dts, mine):
        for n, start, i in mine:
            size = chunks[n][1] if cross else chunks[0][1]
            for dt in dts:
                send(
                    x_ref.at[pl.ds(i, size)], sg.at[me, pl.ds(start, size)], sent.at[0], s_sem.at[n, dt],
                    at(q, f, to_t[dt]),
                )

    def own_copies(mine):
        for n, start, i in mine:
            size = chunks[n][1] if cross else chunks[0][1]
            pltpu.make_async_copy(
                x_hbm.at[pl.ds(i, size)], sg.at[me, pl.ds(start, size)], s_sem.at[n, 0]
            ).start()

    def mine_of(kk):
        return [(n, c, c % own_rows) for n, (c, _) in enumerate(chunks) if c // own_rows == kk]

    if cross:
        for kk in range(P_):
            pl.when(k == kk)(functools.partial(own_copies, mine_of(kk)))
    else:
        size = chunks[0][1]
        mine = [(k * (own_rows // size) + i, k * own_rows + i * size, i * size) for i in range(own_rows // size)]
        if P_ > feeds:
            pl.when(k < feeds)(functools.partial(own_copies, mine))
        else:
            own_copies(mine)
    barrier = pltpu.get_barrier_semaphore()
    column = [at(k, f, tt) for tt in to_t[1:]]
    if cross:
        everyone = column + [at(k, f ^ b, t) for b in bits] + [at(1 - k, f, t)]
    else:
        everyone = peers + [dev for dk in range(1, P_) for dev in plane(lax.rem(k + dk, P_))]
    for dev in everyone:
        pl.semaphore_signal(barrier, inc=1, device_id=dev, device_id_type=MESH)
    for load in loads[:4]:
        load.wait()
    gains[me] = gain_ref[...].astype(jnp.float32)
    lnp[0] = lgain_ref[...] * 0.5
    lnp[1] = lshift_ref[...] * 0.5
    pad[0:head, :] = jnp.zeros((head, C), jnp.float32)
    turn[...] = jnp.zeros_like(turn)
    pl.semaphore_wait(barrier, len(everyone))

    def meet():
        for i, b in enumerate(bits):
            pl.semaphore_signal(meet_sem.at[i], inc=1, device_id=at(k, f ^ b, t), device_id_type=MESH)
            pl.semaphore_wait(meet_sem.at[i], 1)
        pl.semaphore_signal(meet_sem.at[top], inc=1, device_id=at(1 - k, f, t), device_id_type=MESH)

    def give(n, i, start, size, cls, dev):
        send(x_ref.at[pl.ds(i, size)], sg.at[me, pl.ds(start, size)], sent.at[0], s_sem.at[n, cls], dev)
        counts[0] += size

    def introduce(last):
        if cross:
            pl.semaphore_wait(meet_sem.at[top], 1)
        if not last:
            for dev in plane(k + 1):
                send(lnp, lng.at[me], sent.at[0], gain_sem.at[1], dev)

    def greet():
        for dev in peers:
            send(gains.at[me], gains.at[me], sent.at[0], gain_sem.at[0], dev)

    top = len(bits)
    counts = [0]

    def stage(r):
        return 0 if r == 0 else len(bits) - ((r & -r).bit_length() - 1)

    relayed = [r for r in range(F) if not top or stage(r) < top]
    ends = [r for r in range(F) if r not in relayed]

    def kind(r, dt):
        if top and stage(r) == top:
            return len(relayed) * T
        return relayed.index(r) * T + dt

    def forward(buf, sem, n, slot, cls, dev):
        block = buf.at[slot, rows_of(n)]
        send(block, block, sent.at[0], sem.at[n, cls], dev)
        counts[0] += chunks[n][1]

    def arrived(buf, sem, n, slot, cls):
        await_bytes(buf.at[slot, rows_of(n)], sem.at[n, cls])

    def hop(buf, sem, n, lv, dts, ups=every, down=True, over=(), given=False, base=0):
        if top and lv == top:
            await_bytes(buf.at[pl.ds(0, len(ends) * T), rows_of(n)], sem.at[n, kind(ends[0], 0) - base])
            return
        for r in range(F):
            if stage(r) != lv:
                continue
            for dt in dts:
                slot = (f ^ r) * T + from_t[dt]
                arrived(buf, sem, n, slot, kind(r, dt) - base)
                if given and dt == 0:
                    continue
                for b in bits:
                    if b < ((r & -r) or F) and (dt in ups if b == F // 2 else down):
                        forward(buf, sem, n, slot, kind(r ^ b, dt) - base, at(k, f ^ b, t))
                if dt in over:
                    forward(buf, sem, n, slot, kind(r, dt) - base, at(1 - k, f, t))

    def prepare(first):
        if not first:
            await_bytes(lng.at[pl.ds(0, G)], gain_sem.at[1])
        for load in loads[4:]:
            load.wait()
        taps[...] = taps_ref[0].astype(jnp.float32)
        await_bytes(gains.at[pl.ds(0, G - 1)], gain_sem.at[0])
        for s in range(G):
            turn[s : s + 1, :] = gains[s]
        cols = turn[...].T
        for s in range(G):
            rows = pl.ds(s * C, C)
            wcat[rows, :] = (wcat[rows, :].astype(jnp.float32) * cols[:, s : s + 1]).astype(jnp.bfloat16)

    def moments(ref, n):
        R = chunks[n][1]
        turn[0:2, :] = jnp.sum(ref[n], axis=0)
        cols = turn[...].T
        mu = cols[0:R, 0:1] / D
        var = cols[0:R, 1:2] / D - mu * mu
        return mu, lax.rsqrt(var + layer_eps)

    def layer_end(n, slot, mu, rs):
        half = (cg[slot, rows_of(n)].astype(jnp.float32) - mu) * rs * lng[slot, 0] + lng[slot, 1]
        hg[slot, rows_of(n)] = (
            sg[slot, rows_of(n)].astype(jnp.float32) + (half + half * jnp.tanh(half))
        ).astype(jnp.bfloat16)

    def enter(n, swapped):
        await_bytes(sin.at[n, pl.ds(0, G)], sin_sem.at[n])
        mu, rs = moments(sin, n)
        if swapped:
            keep[n, 0, 0 : chunks[n][1], :] = jnp.broadcast_to(mu, (chunks[n][1], C))
            keep[n, 1, 0 : chunks[n][1], :] = jnp.broadcast_to(rs, (chunks[n][1], C))
        for dt in (ENTER if len(ENTER) == T else every):
            slot = f * T + from_t[dt]
            if dt or not zrelay:
                arrived(cg, c_sem, n, slot, dt)
            layer_end(n, slot, mu, rs)
            for b in bits:
                if not (swapped and dt == 0 and b == F // 2):
                    forward(hg, h_sem, n, slot, kind(b, dt) - T, at(k, f ^ b, t))

    def enter_swapped(n):
        slot = (f ^ (F // 2)) * T + t
        arrived(cg, c_sem, n, slot, T)
        layer_end(n, slot, keep[n, 0, 0 : chunks[n][1], :], keep[n, 1, 0 : chunks[n][1], :])
        for b in bits[1:]:
            forward(hg, h_sem, n, slot, kind(F // 2 ^ b, 0) - T, at(k, f ^ b, t))

    def spread(n):
        slot = f * T + t
        arrived(cg, c_sem, n, slot, 0)
        for dz in zrelay:
            forward(cg, c_sem, n, slot, dz, at(k, f, to_t[dz]))

    def project(n, buf):
        start, R = chunks[n]
        blocks = [buf[s, rows_of(n)] for s in range(G)]
        squares = jnp.zeros((R, C), jnp.float32)
        for xb in blocks:
            xf = xb.astype(jnp.float32)
            squares = squares + xf * xf
        scale = lax.rsqrt(jnp.sum(squares, axis=1, keepdims=True) / D + norm_eps)
        both = jnp.dot(jnp.concatenate(blocks, axis=1), wcat[...], preferred_element_type=jnp.float32) * scale
        j = start % LEN
        pad[head + j : head + j + R, :] = both[:, :C] * (0.5 + 0.5 * jnp.tanh(0.5 * both[:, C:]))
        step = 32 if R % 32 == 0 else R
        for r0 in range(0, R, step):
            acc = jnp.zeros((step, C), jnp.float32)
            for w in range(W):
                o = head - (W - 1) + w + j + r0
                acc = acc + pad[o : o + step, :] * taps[w : w + 1, :]
            conv_own[start + r0 : start + r0 + step, :] = acc
        conv = conv_own[start : start + R, :]
        lane = lax.broadcasted_iota(jnp.int32, (R, LEN), 1)
        s1 = jnp.sum(conv, axis=1, keepdims=True)
        s2 = jnp.sum(conv * conv, axis=1, keepdims=True)
        turn[0:R, :] = jnp.where(lane == 0, s1, jnp.where(lane == 1, s2, 0.0))
        return conv, turn[...].T[0:2, :]

    def pass_on(n, first, swapped):
        conv, stat = project(n, sg if first else hg)
        rows = rows_of(n)
        sout[n] = stat
        conv_out[rows, :] = conv.astype(jnp.bfloat16)
        for dev in plane(k + 1):
            send(sout.at[n], sin.at[n, me], sent.at[0], sin_sem.at[n], dev)
        for dt in SEND if len(SEND) == T else every:
            if dt not in zrelay:
                send(conv_out.at[rows], cg.at[me, rows], sent.at[0], c_sem.at[n, dt], at(k + 1, f, to_t[dt]))
        if swapped:
            send(conv_out.at[rows], side.at[rows], sent.at[0], side_sem.at[n], at(k, f ^ (F // 2), t))
        if not first:
            for dt in every:
                send(hg.at[me, rows], sg.at[me, rows], sent.at[0], s_sem.at[n, dt], at(k + 1, f, to_t[dt]))

    def swap_on(n):
        rows = rows_of(n)
        await_bytes(side.at[rows], side_sem.at[n])
        slot = (f ^ (F // 2)) * T + t
        send(side.at[rows], cg.at[slot, rows], sent.at[0], c_sem.at[n, T], at(k + 1, f, t))

    def last_stats(n, first):
        _, stat = project(n, sg if first else hg)
        sfin[n, me] = stat
        for dev in peers:
            send(sfin.at[n, me], sfin.at[n, me], sent.at[0], sfin_sem.at[n], dev)

    def finish(n, first):
        start, R = chunks[n]
        await_bytes(sfin.at[n, pl.ds(0, G - 1)], sfin_sem.at[n])
        mu, rs = moments(sfin, n)
        half = (conv_own[start : start + R, :] - mu) * rs * lnp[0] + lnp[1]
        stream = (sg if first else hg)[me, rows_of(n)]
        new = (stream.astype(jnp.float32) + (half + half * jnp.tanh(half))).astype(jnp.bfloat16)
        owner, i = start // own_rows, start % own_rows
        rows = pl.ds(i, R)
        if owner == P_ - 1:
            out_ref[rows, :] = new
        else:
            new_buf[rows_of(n), :] = new
            send(new_buf.at[rows_of(n)], out_ref.at[rows], sent.at[0], out_sem.at[0], at(owner, f, t))

    def drain(rows, sem):
        full = sg.shape[1]
        while rows >= full:
            m = min(G, rows // full)
            await_bytes(sg.at[pl.ds(0, m)], sem)
            rows -= m * full
        if rows:
            await_bytes(sg.at[0, pl.ds(0, rows)], sem)

    def run(first, last):
        counts[0] = 0
        kk = 0 if first else 1
        ops = []
        for n, (start, size) in enumerate(chunks):
            own = not cross or start // own_rows == kk
            swapped = cross and F > 1 and start >= SWAP
            at_ = functools.partial(when, chunks, own_rows, cross, kk, n)
            x1 = XCARRY if cross else ()
            zero = (0,) if swapped else ()
            if first:
                if own:
                    ops.append((at_("S0"), functools.partial(hop, sg, s_sem, n, 0, every, over=every if cross else (), given=cross)))
                else:
                    ups = tuple(d for d in every if d not in x1)
                    ops.append((at_("S0"), functools.partial(hop, sg, s_sem, n, 0, every, ups)))
                for lv in range(1, top + 1):
                    over = zero if own and lv == 1 else ()
                    ops.append((at_("S%d" % min(lv, 2)), functools.partial(hop, sg, s_sem, n, lv, every, over=over)))
            else:
                if cross and own:
                    ups = tuple(sorted(set(x1 + zero)))
                    ops.append((at_("S0"), functools.partial(hop, sg, s_sem, n, 0, every, ups, False, every, True)))
                    if ups:
                        ops.append((at_("S1"), functools.partial(hop, sg, s_sem, n, 1, ups, (), False, x1)))
                else:
                    ops.append((at_("S0"), functools.partial(hop, sg, s_sem, n, 0, every, (), False)))
                    if swapped:
                        ops.append((at_("S1"), functools.partial(hop, sg, s_sem, n, 1, (0,), (), False)))
                if zrelay:
                    ops.append((at_("C00"), functools.partial(spread, n)))
                ops.append((at_("ent"), functools.partial(enter, n, swapped)))
                if swapped:
                    ops.append((at_("ent2"), functools.partial(enter_swapped, n)))
                for lv in range(1, top + 1):
                    dts = every[1:] if swapped and lv == 1 else every
                    ops.append((at_("C%d" % min(lv, 2)), functools.partial(hop, hg, h_sem, n, lv, dts, base=T)))
            if n == 0:
                ops.append((at_("prep"), functools.partial(prepare, first)))
            if last:
                ops.append((at_("step"), functools.partial(last_stats, n, first)))
                ops.append((at_("fin"), functools.partial(finish, n, first)))
            else:
                ops.append((at_("step"), functools.partial(pass_on, n, first, swapped)))
                if swapped:
                    ops.append((at_("swap"), functools.partial(swap_on, n)))
        if cross:
            for entry in mine_of(kk):
                feed(kk, FEED, [entry])
                n, start, i = entry
                size = chunks[n][1]
                swapped = start >= SWAP
                for b in bits:
                    if (first or 0 in XCARRY or swapped) if b == F // 2 else first:
                        give(n, i, start, size, kind(b, 0), at(k, f ^ b, t))
                give(n, i, start, size, 0, at(1 - k, f, t))
            meet()
        greet()
        soon = min(op[0] for op in ops)
        ops.append((soon + 1e-6, functools.partial(introduce, last)))
        for _, op in sorted(ops, key=lambda op: op[0]):
            op()
        drain(counts[0], sent.at[0])
        total = sg.shape[1]
        await_bytes(gains.at[pl.ds(0, G - 1)], sent.at[0])
        if last:
            await_bytes(sfin.at[:, pl.ds(0, G - 1)], sent.at[0])
            if P_ > 1:
                drain(total - own_rows, sent.at[0])
        else:
            await_bytes(sin.at[:, pl.ds(0, G)], sent.at[0])
            await_bytes(lng.at[pl.ds(0, G)], sent.at[0])
            drain(total * (T - len(zrelay)), sent.at[0])
            if cross and F > 1:
                drain(2 * sum(c[1] for c in chunks if c[0] >= SWAP), sent.at[0])
            if not first:
                drain(total * T, sent.at[0])

    if not cross:
        for q in range(feeds):
            feed(q, range(1, T), mine)
            if P_ > 1:
                pl.when(k != q)(functools.partial(feed, q, [0], mine))
    if P_ == 1:
        run(True, True)
    else:
        pl.when(k == 0)(lambda: run(True, False))
        pl.when(k == P_ - 1)(lambda: run(False, True))
        if P_ > 2:
            pl.when((k > 0) & (k < P_ - 1))(lambda: run(False, False))

    drain(own_rows * (T - 1 if cross else feeds * T - 1), sent.at[0])
    if P_ > 2:
        pl.when(k >= feeds)(lambda: await_bytes(x_ref, sent.at[0]))
    if P_ > 1:
        pl.when(k < P_ - 1)(lambda: await_bytes(out_ref, out_sem.at[0]))


def plan(sizes, own_rows):
    if sizes[0] == 2 and sizes[2] & (sizes[2] - 1) == 0 and all(sum(split) == own_rows for split in SPLITS):
        rows = [size for split in SPLITS for size in split]
        return [(sum(rows[:i]), size) for i, size in enumerate(rows)], True
    size = min(64, own_rows)
    return [(i * size, size) for i in range(own_rows * sizes[0] // size)], False


def when(chunks, own_rows, cross, kk, n, op):
    if cross and TIMES:
        if op == "prep":
            return TIMES[kk]["C00" if kk else "S1"][0] - 0.01
        return TIMES[kk][op][n]
    start, size = chunks[n]
    late = start + size
    mine = late - start // own_rows * own_rows if cross else late
    own = not cross or start // own_rows == kk
    base = 6.6 + 1.4 * late / 64
    s0 = 3 + 0.7 * mine / 64 if own else 5.5 + 0.7 * mine / 64
    s1 = 5.5 + 1.4 * mine / 64 if own else 11.5 + 0.8 * mine / 64
    first = {"S0": s0, "S1": s1, "S2": s1 + 1, "step": s1 + 1.1, "prep": s1 + 1.05, "swap": s1 + 4, "fin": s1 + 6}
    later = {
        "S0": s0, "S1": s1, "C00": base + 3, "ent": base + 6, "ent2": base + 8, "C1": base + 9, "C2": base + 10,
        "prep": base + 2.9, "step": base + 10.1, "swap": base + 13, "fin": base + 15,
    }
    return (later if kk else first)[op]


def local(sizes, inputs, norm_gain, w_value, w_gate, w_taps, ln_gain, ln_shift):
    P_, F, T = sizes
    G = F * T
    own_rows, C = inputs.shape
    TOK = own_rows * P_
    chunks, _ = plan(sizes, own_rows)
    NC = len(chunks)
    D = w_value.shape[1]
    W = w_taps.shape[1]
    head = -(-(W - 1) // 8) * 8
    operands = (inputs, norm_gain, w_value, w_gate, w_taps, ln_gain, ln_shift)
    dma = pltpu.SemaphoreType.DMA
    f32, bf16 = jnp.float32, jnp.bfloat16
    V = pltpu.VMEM
    return pl.pallas_call(
        functools.partial(kernel, sizes),
        out_shape=pltpu.VMEM((own_rows, C), bf16),
        in_specs=[pl.BlockSpec(memory_space=pl.ANY)] * 7,
        out_specs=pl.BlockSpec(memory_space=pltpu.VMEM),
        scratch_shapes=[
            V(inputs.shape, bf16), V(norm_gain.shape, bf16), V((D, 2 * C), bf16), V(w_taps.shape, bf16),
            V(ln_gain.shape, f32), V(ln_shift.shape, f32),
            dma((len(operands),)),
            V((G, TOK, C), bf16), V((G, TOK, C), bf16), V((G, TOK, C), bf16),
            V((G, 1, C), f32), V((G, 2, 1, C), f32),
            V((NC, G, 2, LEN), f32), V((NC, G, 2, LEN), f32), V((NC, 2, LEN), f32),
            V((LEN + head, C), f32), V((W, C), f32),
            V((TOK, C), f32), V((TOK, C), bf16), V((NC, 2, LEN, C), f32), V((2, 1, C), f32), V((TOK, C), bf16),
            V((LEN, LEN), f32),
            dma((NC, T * F)) if F & (F - 1) else dma((NC, max(F // 2, 1) * T + 1)),
            dma((NC, T + 1)), dma((NC, max(F // 2 - 1, 0) * T + 1)), dma((NC,)), dma((NC,)), dma((2,)), dma((1,)),
            dma((1,)), V((TOK, C), bf16), dma((NC,)), pltpu.SemaphoreType.REGULAR((4,)),
        ],
        compiler_params=pltpu.CompilerParams(collective_id=0, has_side_effects=True),
    )(*operands)


def solution(mesh):
    sizes = (mesh.shape["pp"], mesh.shape["fs"], mesh.shape["tp"])
    in_specs = (
        P("pp", ("fs", "tp")),
        P("pp", ("fs", "tp")),
        P("pp", None, ("fs", "tp")),
        P("pp", None, ("fs", "tp")),
        P("pp", None, ("fs", "tp")),
        P("pp", ("fs", "tp")),
        P("pp", ("fs", "tp")),
    )
    out_specs = P("pp", ("fs", "tp"))
    return jax.shard_map(
        functools.partial(local, sizes), mesh=mesh, in_specs=in_specs, out_specs=out_specs,
        check_vma=False,
    )
```

```python
import functools

import jax
import jax.numpy as jnp
from jax import lax
from jax.experimental import pallas as pl
from jax.experimental.pallas import tpu as pltpu
from jax.sharding import PartitionSpec as P

LEN = 128
SPLITS = ((128, 128), (128, 128))
FEED = (1, 2, 3)
SEND = (3, 0, 2, 1)
ENTER = (0, 3, 1, 2)
XCARRY = (1, 2, 3)
ZRELAY = (1, 2)
SWAP = 256
TIMES = (
    {"S0": (-0.48, 4.35, 10.17, 11.39), "S1": (6.67, 11.13, 17.25, 20.33), "S2": (8.5, 15.39, 18.61, 20.55), "step": (8.5, 15.39, 18.61, 20.55), "swap": (0, 0, 26.5, 26.88)},
    {"S0": (10.67, 16.26, 7.57, 7.57), "C00": (16.08, 17.31, 18.47, 19.95), "ent": (18.0, 19.3, 21.72, 24.23), "C1": (21.04, 25.35, 26.83, 31.69), "C2": (21.81, 26.26, 31.37, 33.41), "step": (21.81, 26.27, 31.37, 33.42), "fin": (32.83, 34.11, 38.98, 44.31), "S1": (0, 0, 8.63, 11.78), "ent2": (0, 0, 29.86, 28.1)},
)


norm_eps = 1e-06
layer_eps = 1e-05
MESH = pl.DeviceIdType.MESH


def kernel(
    sizes,
    x_hbm,
    gain_hbm,
    wv_hbm,
    wg_hbm,
    taps_hbm,
    lgain_hbm,
    lshift_hbm,
    out_ref,
    x_ref,
    gain_ref,
    wcat,
    taps_ref,
    lgain_ref,
    lshift_ref,
    load_sem,
    sg,
    cg,
    hg,
    gains,
    lng,
    sin,
    sfin,
    sout,
    pad,
    taps,
    conv_own,
    conv_out,
    keep,
    lnp,
    new_buf,
    turn,
    s_sem,
    c_sem,
    h_sem,
    sin_sem,
    sfin_sem,
    gain_sem,
    out_sem,
    sent,
    side,
    side_sem,
    meet_sem,
):
    P_, F, T = sizes
    G = F * T
    k, f, t = lax.axis_index("pp"), lax.axis_index("fs"), lax.axis_index("tp")
    C = conv_own.shape[1]
    D = wcat.shape[0]
    W = taps.shape[0]
    own_rows = x_ref.shape[0]
    head = pad.shape[0] - LEN
    me = f * T + t
    feeds = min(2, P_)

    loads = [
        pltpu.make_async_copy(a, b, load_sem.at[n])
        for n, (a, b) in enumerate(
            [
                (x_hbm, x_ref), (gain_hbm, gain_ref), (lgain_hbm, lgain_ref), (lshift_hbm, lshift_ref),
                (taps_hbm, taps_ref),
                (wv_hbm.at[0], wcat.at[:, pl.ds(0, C)]), (wg_hbm.at[0], wcat.at[:, pl.ds(C, C)]),
            ]
        )
    ]
    for load in loads:
        load.start()

    if T & (T - 1) == 0:
        to_t = [t] + [t ^ d for d in range(1, T)]
        from_t = to_t
    else:
        to_t = [lax.rem(t + d, T) for d in range(T)]
        from_t = [lax.rem(t + T - d, T) for d in range(T)]

    def at(kk, ff, tt):
        return {"pp": kk, "fs": ff, "tp": tt}

    def send(src, dst, s_sem_, r_sem, dev):
        pltpu.make_async_remote_copy(
            src_ref=src, dst_ref=dst, send_sem=s_sem_, recv_sem=r_sem, device_id=dev, device_id_type=MESH
        ).start()

    def await_bytes(ref, sem):
        pltpu.make_async_copy(ref, ref, sem).wait()

    peers = [at(k, lax.rem(f + df, F), to_t[dt]) for dt in range(T - 1, -1, -1) for df in range(F) if df or dt]

    def plane(kk):
        return [at(kk, lax.rem(f + df, F), to_t[dt]) for dt in range(T - 1, -1, -1) for df in range(F)]

    bits = []
    b = F // 2
    while b:
        bits.append(b)
        b //= 2
    pow2 = T & (T - 1) == 0
    every = tuple(range(T))
    chunks, cross = plan(sizes, own_rows)
    NCH = len(chunks)
    lead = sum(start < SWAP for start, _ in chunks)
    zrelay = ZRELAY if pow2 and T == 4 else ()

    def rows_of(n):
        return pl.ds(chunks[n][0], chunks[n][1])

    def feed(q, dts, mine):
        for n, start, i in mine:
            size = chunks[n][1] if cross else chunks[0][1]
            for dt in dts:
                send(
                    x_ref.at[pl.ds(i, size)], sg.at[me, pl.ds(start, size)], sent.at[0], s_sem.at[n, dt],
                    at(q, f, to_t[dt]),
                )

    def own_copies(mine):
        for n, start, i in mine:
            size = chunks[n][1] if cross else chunks[0][1]
            pltpu.make_async_copy(
                x_hbm.at[pl.ds(i, size)], sg.at[me, pl.ds(start, size)], s_sem.at[n, 0]
            ).start()

    def mine_of(kk):
        return [(n, c, c % own_rows) for n, (c, _) in enumerate(chunks) if c // own_rows == kk]

    if cross:
        for kk in range(P_):
            pl.when(k == kk)(functools.partial(own_copies, mine_of(kk)))
    else:
        size = chunks[0][1]
        mine = [(k * (own_rows // size) + i, k * own_rows + i * size, i * size) for i in range(own_rows // size)]
        if P_ > feeds:
            pl.when(k < feeds)(functools.partial(own_copies, mine))
        else:
            own_copies(mine)
    barrier = pltpu.get_barrier_semaphore()
    column = [at(k, f, tt) for tt in to_t[1:]]
    if cross:
        everyone = column + [at(k, f ^ b, t) for b in bits] + [at(1 - k, f, t)]
    else:
        everyone = peers + [dev for dk in range(1, P_) for dev in plane(lax.rem(k + dk, P_))]
    for dev in everyone:
        pl.semaphore_signal(barrier, inc=1, device_id=dev, device_id_type=MESH)
    for load in loads[:4]:
        load.wait()
    gains[me] = gain_ref[...].astype(jnp.float32)
    lnp[0] = lgain_ref[...] * 0.5
    lnp[1] = lshift_ref[...] * 0.5
    pad[0:head, :] = jnp.zeros((head, C), jnp.float32)
    turn[...] = jnp.zeros_like(turn)
    pl.semaphore_wait(barrier, len(everyone))

    def meet():
        for i, b in enumerate(bits):
            pl.semaphore_signal(meet_sem.at[i], inc=1, device_id=at(k, f ^ b, t), device_id_type=MESH)
            pl.semaphore_wait(meet_sem.at[i], 1)
        pl.semaphore_signal(meet_sem.at[top], inc=1, device_id=at(1 - k, f, t), device_id_type=MESH)

    def give(n, i, start, size, cls, dev):
        send(x_ref.at[pl.ds(i, size)], sg.at[me, pl.ds(start, size)], sent.at[0], s_sem.at[n, cls], dev)
        counts[0] += size

    def introduce(last):
        if cross:
            pl.semaphore_wait(meet_sem.at[top], 1)
        if not last:
            for dev in plane(k + 1):
                send(lnp, lng.at[me], sent.at[0], gain_sem.at[1], dev)

    def greet():
        for dev in peers:
            send(gains.at[me], gains.at[me], sent.at[0], gain_sem.at[0], dev)

    top = len(bits)
    counts = [0]

    def stage(r):
        return 0 if r == 0 else len(bits) - ((r & -r).bit_length() - 1)

    relayed = [r for r in range(F) if not top or stage(r) < top]
    ends = [r for r in range(F) if r not in relayed]

    def kind(r, dt):
        if top and stage(r) == top:
            return len(relayed) * T
        return relayed.index(r) * T + dt

    def forward(buf, sem, n, slot, cls, dev):
        block = buf.at[slot, rows_of(n)]
        send(block, block, sent.at[0], sem.at[n, cls], dev)
        counts[0] += chunks[n][1]

    def arrived(buf, sem, n, slot, cls):
        await_bytes(buf.at[slot, rows_of(n)], sem.at[n, cls])

    def hop(buf, sem, n, lv, dts, ups=every, down=True, over=(), given=False, base=0):
        if top and lv == top:
            await_bytes(buf.at[pl.ds(0, len(ends) * T), rows_of(n)], sem.at[n, kind(ends[0], 0) - base])
            return
        for r in range(F):
            if stage(r) != lv:
                continue
            for dt in dts:
                slot = (f ^ r) * T + from_t[dt]
                arrived(buf, sem, n, slot, kind(r, dt) - base)
                if given and dt == 0:
                    continue
                for b in bits:
                    if b < ((r & -r) or F) and (dt in ups if b == F // 2 else down):
                        forward(buf, sem, n, slot, kind(r ^ b, dt) - base, at(k, f ^ b, t))
                if dt in over:
                    forward(buf, sem, n, slot, kind(r, dt) - base, at(1 - k, f, t))

    def prepare(first):
        if not first:
            await_bytes(lng.at[pl.ds(0, G)], gain_sem.at[1])
        for load in loads[4:]:
            load.wait()
        taps[...] = taps_ref[0].astype(jnp.float32)
        await_bytes(gains.at[pl.ds(0, G - 1)], gain_sem.at[0])
        for s in range(G):
            turn[s : s + 1, :] = gains[s]
        cols = turn[...].T
        for s in range(G):
            rows = pl.ds(s * C, C)
            wcat[rows, :] = (wcat[rows, :].astype(jnp.float32) * cols[:, s : s + 1]).astype(jnp.bfloat16)

    def moments(ref, n):
        R = chunks[n][1]
        turn[0:2, :] = jnp.sum(ref[n], axis=0)
        cols = turn[...].T
        mu = cols[0:R, 0:1] / D
        var = cols[0:R, 1:2] / D - mu * mu
        return mu, lax.rsqrt(var + layer_eps)

    def layer_end(n, slot, mu, rs):
        half = (cg[slot, rows_of(n)].astype(jnp.float32) - mu) * rs * lng[slot, 0] + lng[slot, 1]
        hg[slot, rows_of(n)] = (
            sg[slot, rows_of(n)].astype(jnp.float32) + (half + half * jnp.tanh(half))
        ).astype(jnp.bfloat16)

    def enter(n, swapped):
        await_bytes(sin.at[n, pl.ds(0, G)], sin_sem.at[n])
        mu, rs = moments(sin, n)
        if swapped:
            keep[n, 0, 0 : chunks[n][1], :] = jnp.broadcast_to(mu, (chunks[n][1], C))
            keep[n, 1, 0 : chunks[n][1], :] = jnp.broadcast_to(rs, (chunks[n][1], C))
        for dt in (ENTER if len(ENTER) == T else every):
            slot = f * T + from_t[dt]
            if dt or not zrelay:
                arrived(cg, c_sem, n, slot, dt)
            layer_end(n, slot, mu, rs)
            for b in bits:
                if not (swapped and dt == 0 and b == F // 2):
                    forward(hg, h_sem, n, slot, kind(b, dt) - T, at(k, f ^ b, t))

    def enter_swapped(n):
        slot = (f ^ (F // 2)) * T + t
        arrived(cg, c_sem, n, slot, T)
        layer_end(n, slot, keep[n, 0, 0 : chunks[n][1], :], keep[n, 1, 0 : chunks[n][1], :])
        for b in bits[1:]:
            forward(hg, h_sem, n, slot, kind(F // 2 ^ b, 0) - T, at(k, f ^ b, t))

    def spread(n):
        slot = f * T + t
        arrived(cg, c_sem, n, slot, 0)
        for dz in zrelay:
            forward(cg, c_sem, n, slot, dz, at(k, f, to_t[dz]))

    def project(n, buf):
        start, R = chunks[n]
        blocks = [buf[s, rows_of(n)] for s in range(G)]
        squares = jnp.zeros((R, C), jnp.float32)
        for xb in blocks:
            xf = xb.astype(jnp.float32)
            squares = squares + xf * xf
        scale = lax.rsqrt(jnp.sum(squares, axis=1, keepdims=True) / D + norm_eps)
        both = jnp.dot(jnp.concatenate(blocks, axis=1), wcat[...], preferred_element_type=jnp.float32) * scale
        j = start % LEN
        pad[head + j : head + j + R, :] = both[:, :C] * (0.5 + 0.5 * jnp.tanh(0.5 * both[:, C:]))
        step = 32 if R % 32 == 0 else R
        for r0 in range(0, R, step):
            acc = jnp.zeros((step, C), jnp.float32)
            for w in range(W):
                o = head - (W - 1) + w + j + r0
                acc = acc + pad[o : o + step, :] * taps[w : w + 1, :]
            conv_own[start + r0 : start + r0 + step, :] = acc
        conv = conv_own[start : start + R, :]
        lane = lax.broadcasted_iota(jnp.int32, (R, LEN), 1)
        s1 = jnp.sum(conv, axis=1, keepdims=True)
        s2 = jnp.sum(conv * conv, axis=1, keepdims=True)
        turn[0:R, :] = jnp.where(lane == 0, s1, jnp.where(lane == 1, s2, 0.0))
        return conv, turn[...].T[0:2, :]

    def pass_on(n, first, swapped):
        conv, stat = project(n, sg if first else hg)
        rows = rows_of(n)
        sout[n] = stat
        conv_out[rows, :] = conv.astype(jnp.bfloat16)
        for dev in plane(k + 1):
            send(sout.at[n], sin.at[n, me], sent.at[0], sin_sem.at[n], dev)
        for dt in SEND if len(SEND) == T else every:
            if dt not in zrelay:
                send(conv_out.at[rows], cg.at[me, rows], sent.at[0], c_sem.at[n, dt], at(k + 1, f, to_t[dt]))
        if swapped:
            send(conv_out.at[rows], side.at[rows], sent.at[0], side_sem.at[n - lead], at(k, f ^ (F // 2), t))
        if not first:
            for dt in every:
                send(hg.at[me, rows], sg.at[me, rows], sent.at[0], s_sem.at[n, dt], at(k + 1, f, to_t[dt]))

    def swap_on(n):
        rows = rows_of(n)
        await_bytes(side.at[rows], side_sem.at[n - lead])
        slot = (f ^ (F // 2)) * T + t
        send(side.at[rows], cg.at[slot, rows], sent.at[0], c_sem.at[n, T], at(k + 1, f, t))

    def last_stats(n, first):
        _, stat = project(n, sg if first else hg)
        sfin[n, me] = stat
        for dev in peers:
            send(sfin.at[n, me], sfin.at[n, me], sent.at[0], sfin_sem.at[n], dev)

    def finish(n, first):
        start, R = chunks[n]
        await_bytes(sfin.at[n, pl.ds(0, G - 1)], sfin_sem.at[n])
        mu, rs = moments(sfin, n)
        half = (conv_own[start : start + R, :] - mu) * rs * lnp[0] + lnp[1]
        stream = (sg if first else hg)[me, rows_of(n)]
        new = (stream.astype(jnp.float32) + (half + half * jnp.tanh(half))).astype(jnp.bfloat16)
        owner, i = start // own_rows, start % own_rows
        rows = pl.ds(i, R)
        if owner == P_ - 1:
            out_ref[rows, :] = new
        else:
            new_buf[rows_of(n), :] = new
            send(new_buf.at[rows_of(n)], out_ref.at[rows], sent.at[0], out_sem.at[0], at(owner, f, t))

    def drain(rows, sem):
        full = sg.shape[1]
        while rows >= full:
            m = min(G, rows // full)
            await_bytes(sg.at[pl.ds(0, m)], sem)
            rows -= m * full
        if rows:
            await_bytes(sg.at[0, pl.ds(0, rows)], sem)

    def run(first, last):
        counts[0] = 0
        kk = 0 if first else 1
        ops = []
        for n, (start, size) in enumerate(chunks):
            own = not cross or start // own_rows == kk
            swapped = cross and F > 1 and start >= SWAP
            at_ = functools.partial(when, chunks, own_rows, cross, kk, n)
            x1 = XCARRY if cross else ()
            zero = (0,) if swapped else ()
            if first:
                if own:
                    ops.append((at_("S0"), functools.partial(hop, sg, s_sem, n, 0, every, over=every if cross else (), given=cross)))
                else:
                    ups = tuple(d for d in every if d not in x1)
                    ops.append((at_("S0"), functools.partial(hop, sg, s_sem, n, 0, every, ups)))
                for lv in range(1, top + 1):
                    over = zero if own and lv == 1 else ()
                    ops.append((at_("S%d" % min(lv, 2)), functools.partial(hop, sg, s_sem, n, lv, every, over=over)))
            else:
                if cross and own:
                    ups = tuple(sorted(set(x1 + zero)))
                    ops.append((at_("S0"), functools.partial(hop, sg, s_sem, n, 0, every, ups, False, every, True)))
                    if ups:
                        ops.append((at_("S1"), functools.partial(hop, sg, s_sem, n, 1, ups, (), False, x1)))
                else:
                    ops.append((at_("S0"), functools.partial(hop, sg, s_sem, n, 0, every, (), False)))
                    if swapped:
                        ops.append((at_("S1"), functools.partial(hop, sg, s_sem, n, 1, (0,), (), False)))
                if zrelay:
                    ops.append((at_("C00"), functools.partial(spread, n)))
                ops.append((at_("ent"), functools.partial(enter, n, swapped)))
                if swapped:
                    ops.append((at_("ent2"), functools.partial(enter_swapped, n)))
                for lv in range(1, top + 1):
                    dts = every[1:] if swapped and lv == 1 else every
                    ops.append((at_("C%d" % min(lv, 2)), functools.partial(hop, hg, h_sem, n, lv, dts, base=T)))
            if n == 0:
                ops.append((at_("prep"), functools.partial(prepare, first)))
            if last:
                ops.append((at_("step"), functools.partial(last_stats, n, first)))
                ops.append((at_("fin"), functools.partial(finish, n, first)))
            else:
                ops.append((at_("step"), functools.partial(pass_on, n, first, swapped)))
                if swapped:
                    ops.append((at_("swap"), functools.partial(swap_on, n)))
        if cross:
            for entry in mine_of(kk):
                feed(kk, FEED, [entry])
                n, start, i = entry
                size = chunks[n][1]
                swapped = start >= SWAP
                for b in bits:
                    if (first or 0 in XCARRY or swapped) if b == F // 2 else first:
                        give(n, i, start, size, kind(b, 0), at(k, f ^ b, t))
                give(n, i, start, size, 0, at(1 - k, f, t))
            meet()
        greet()
        soon = min(op[0] for op in ops)
        ops.append((soon + 1e-6, functools.partial(introduce, last)))
        for _, op in sorted(ops, key=lambda op: op[0]):
            op()
        drain(counts[0], sent.at[0])
        total = sg.shape[1]
        await_bytes(gains.at[pl.ds(0, G - 1)], sent.at[0])
        if last:
            await_bytes(sfin.at[:, pl.ds(0, G - 1)], sent.at[0])
            if P_ > 1:
                drain(total - own_rows, sent.at[0])
        else:
            await_bytes(sin.at[:, pl.ds(0, G)], sent.at[0])
            await_bytes(lng.at[pl.ds(0, G)], sent.at[0])
            drain(total * (T - len(zrelay)), sent.at[0])
            if cross and F > 1:
                drain(2 * sum(c[1] for c in chunks if c[0] >= SWAP), sent.at[0])
            if not first:
                drain(total * T, sent.at[0])

    if not cross:
        for q in range(feeds):
            feed(q, range(1, T), mine)
            if P_ > 1:
                pl.when(k != q)(functools.partial(feed, q, [0], mine))
    if P_ == 1:
        run(True, True)
    else:
        pl.when(k == 0)(lambda: run(True, False))
        pl.when(k == P_ - 1)(lambda: run(False, True))
        if P_ > 2:
            pl.when((k > 0) & (k < P_ - 1))(lambda: run(False, False))

    drain(own_rows * (T - 1 if cross else feeds * T - 1), sent.at[0])
    if P_ > 2:
        pl.when(k >= feeds)(lambda: await_bytes(x_ref, sent.at[0]))
    if P_ > 1:
        pl.when(k < P_ - 1)(lambda: await_bytes(out_ref, out_sem.at[0]))


def plan(sizes, own_rows):
    if sizes[0] == 2 and sizes[2] & (sizes[2] - 1) == 0 and all(sum(split) == own_rows for split in SPLITS):
        rows = [size for split in SPLITS for size in split]
        return [(sum(rows[:i]), size) for i, size in enumerate(rows)], True
    size = min(64, own_rows)
    return [(i * size, size) for i in range(own_rows * sizes[0] // size)], False


def when(chunks, own_rows, cross, kk, n, op):
    if cross and TIMES:
        if op == "prep":
            return TIMES[kk]["C00" if kk else "S1"][0] - 0.01
        return TIMES[kk][op][n]
    start, size = chunks[n]
    late = start + size
    mine = late - start // own_rows * own_rows if cross else late
    own = not cross or start // own_rows == kk
    base = 6.6 + 1.4 * late / 64
    s0 = 3 + 0.7 * mine / 64 if own else 5.5 + 0.7 * mine / 64
    s1 = 5.5 + 1.4 * mine / 64 if own else 11.5 + 0.8 * mine / 64
    first = {"S0": s0, "S1": s1, "S2": s1 + 1, "step": s1 + 1.1, "prep": s1 + 1.05, "swap": s1 + 4, "fin": s1 + 6}
    later = {
        "S0": s0, "S1": s1, "C00": base + 3, "ent": base + 6, "ent2": base + 8, "C1": base + 9, "C2": base + 10,
        "prep": base + 2.9, "step": base + 10.1, "swap": base + 13, "fin": base + 15,
    }
    return (later if kk else first)[op]


def local(sizes, inputs, norm_gain, w_value, w_gate, w_taps, ln_gain, ln_shift):
    P_, F, T = sizes
    G = F * T
    own_rows, C = inputs.shape
    TOK = own_rows * P_
    chunks, _ = plan(sizes, own_rows)
    NC = len(chunks)
    D = w_value.shape[1]
    W = w_taps.shape[1]
    head = -(-(W - 1) // 8) * 8
    operands = (inputs, norm_gain, w_value, w_gate, w_taps, ln_gain, ln_shift)
    dma = pltpu.SemaphoreType.DMA
    f32, bf16 = jnp.float32, jnp.bfloat16
    V = pltpu.VMEM
    return pl.pallas_call(
        functools.partial(kernel, sizes),
        out_shape=pltpu.VMEM((own_rows, C), bf16),
        in_specs=[pl.BlockSpec(memory_space=pl.ANY)] * 7,
        out_specs=pl.BlockSpec(memory_space=pltpu.VMEM),
        scratch_shapes=[
            V(inputs.shape, bf16), V(norm_gain.shape, bf16), V((D, 2 * C), bf16), V(w_taps.shape, bf16),
            V(ln_gain.shape, f32), V(ln_shift.shape, f32),
            dma((len(operands),)),
            V((G, TOK, C), bf16), V((G, TOK, C), bf16), V((G, TOK, C), bf16),
            V((G, 1, C), f32), V((G, 2, 1, C), f32),
            V((NC, G, 2, LEN), f32), V((NC, G, 2, LEN), f32), V((NC, 2, LEN), f32),
            V((LEN + head, C), f32), V((W, C), f32),
            V((TOK, C), f32), V((TOK, C), bf16), V((NC, 2, LEN, C), f32), V((2, 1, C), f32), V((TOK, C), bf16),
            V((LEN, LEN), f32),
            dma((NC, T * F)) if F & (F - 1) else dma((NC, max(F // 2, 1) * T + 1)),
            dma((NC, T + 1)), dma((NC, max(F // 2 - 1, 0) * T + 1)), dma((NC,)), dma((NC,)), dma((2,)), dma((1,)),
            dma((1,)), V((TOK, C), bf16), dma((max(sum(c[0] >= SWAP for c in chunks), 1),)), pltpu.SemaphoreType.REGULAR((max(F.bit_length(), 1),)),
        ],
        compiler_params=pltpu.CompilerParams(collective_id=0, has_side_effects=True),
    )(*operands)


def solution(mesh):
    sizes = (mesh.shape["pp"], mesh.shape["fs"], mesh.shape["tp"])
    in_specs = (
        P("pp", ("fs", "tp")),
        P("pp", ("fs", "tp")),
        P("pp", None, ("fs", "tp")),
        P("pp", None, ("fs", "tp")),
        P("pp", None, ("fs", "tp")),
        P("pp", ("fs", "tp")),
        P("pp", ("fs", "tp")),
    )
    out_specs = P("pp", ("fs", "tp"))
    return jax.shard_map(
        functools.partial(local, sizes), mesh=mesh, in_specs=in_specs, out_specs=out_specs,
        check_vma=False,
    )
```
